256 devices in a mesh: ep: 32 (over z, x), tp: 8 (over y, core).
Axes of the slice: x: 4, y: 4, z: 8, core: 2. Of those that a mesh axis runs over, the one named last changes fastest.
Arguments:
- out_gate: bfloat16 [32768, 2048], P(('ep', 'tp')), may hold values from -6 to 6
- in_gate: bfloat16 [32768, 2048], P(('ep', 'tp')), may hold values from -6 to 6
- values: bfloat16 [32768, 2048], P(('ep', 'tp')), may hold values from -6 to 6
- conv_taps: float32 [3, 2048], replicated, may hold values from -4 to 4
- out_weight: bfloat16 [2048, 2048], P(None, 'tp'), may hold values from -0.125 to 0.125
- expert_input: bfloat16 [65536, 2048], P(('ep', 'tp')), may hold values from -6 to 6
- norm_gain: float32 [2048], replicated, may hold values from 0.1 to 1.9
- expert_ids: int32 [65536, 2], P(('ep', 'tp')), may hold values from 0 to 31, all different within a row; in each aligned block of 256 rows (0 to 255, 256 to 511, ...) at most 32 rows name the same one
- route_logits: float32 [65536, 2], P(('ep', 'tp')), may hold values from -8 to 8
- group_share: float32 [65536], P(('ep', 'tp')), may hold values from 0.3 to 1
- gate_weight: bfloat16 [32, 2048, 512], P('ep'), may hold values from -0.125 to 0.125
- up_weight: bfloat16 [32, 2048, 512], P('ep'), may hold values from -0.125 to 0.125
- down_weight: bfloat16 [32, 512, 2048], P('ep'), may hold values from -0.25 to 0.25
Outputs:
- mixer_out: bfloat16 [32768, 2048], P(('ep', 'tp'))
- expert_mix: bfloat16 [65536, 2048], P(('ep', 'tp'))
The draws below stay inside these ranges and needn't reach their ends.
Inputs may be any that keep to these rules, and one draw needn't show every extreme that they name: `expert_ids`: each row names 2 different experts. Within the rows of one device (aligned blocks of 256 rows) no expert is named by more than 32 rows, a bound that some block reaches.
All inputs are finite; a program needn't handle non-finite values.
Results may differ from the reference program's by a relative error of at most 0.0071.
Values may be sent and summed in bfloat16 or wider, within the bound.
A program may use at most 128 MiB of HBM per device.

```python
import math
import jax
import jax.numpy as jnp
import numpy as np
from jax import lax

D = 2048
F = 512
EXPERTS = 32
TOP = 2
CONV = 3
SEQS = 1
TOK_B = 256
TOKENS_A = 32768
TOKENS_B = 65536
CAP = 32
N_EP = 32
N_TP = 8


def levels(stream_key, dims, pieces, least, high):
    def one(axis_at, blocks):
        heights = jax.random.uniform(jax.random.fold_in(jax.random.fold_in(stream_key, 6), axis_at), (blocks,), jnp.float32, least / len(pieces), high / len(pieces))
        return jnp.repeat(jnp.exp(heights), dims[axis_at] // blocks).reshape((-1,) + (1,) * (len(dims) - axis_at - 1))

    loudness = one(*pieces[0])
    for cut in pieces[1:]:
        loudness = loudness * one(*cut)
    return loudness


def shared_out(stream_key, own, number, rows, amount, top, reach, slope):
    ranking = jax.random.permutation(stream_key, amount)
    heavy_load, common = shares(amount, rows * top, reach, slope, True), shares(amount, rows * top, reach, slope, False)
    places = jnp.arange(amount)

    def named(lengths, rotation):
        used = int((lengths > 0).sum())
        fixed = max(1, used // 4)
        shifted = fixed + (places - fixed + rotation * (used - fixed)) % max(1, amount - fixed)
        return jnp.zeros((amount,), jnp.int32).at[ranking[jnp.where(places < fixed, places, shifted)]].set(jnp.asarray(lengths, jnp.int32))

    lengths = jnp.where(number % 4 == 0, named(heavy_load, number // 4), named(common, number - number // 4 - 1))
    mixed = jax.random.permutation(jax.random.fold_in(own, 3), amount)
    giver, receiver = mixed[0:amount // 2 * 2:2], mixed[1:amount // 2 * 2:2]
    room = jnp.minimum(lengths[giver] - 1, reach - lengths[receiver]) // 2
    room = jnp.where((giver == ranking[0]) | (receiver == ranking[0]) | (lengths[receiver] == 0), 0, jnp.maximum(room, 0))
    shifted = jax.random.randint(jax.random.fold_in(own, 4), (amount // 2,), 0, 1 << 20) % (room + 1)
    lengths = lengths.at[giver].add(-shifted).at[receiver].add(shifted)
    items = jnp.searchsorted(jnp.cumsum(lengths), jnp.arange(rows * top), side="right").astype(jnp.int32)
    listing = items.reshape(top, rows).T
    listing = listing[jax.random.permutation(jax.random.fold_in(own, 1), rows)]
    rotation = jax.random.randint(jax.random.fold_in(own, 2), (rows, 1), 0, top)
    return jnp.take_along_axis(listing, (jnp.arange(top)[None, :] + rotation) % top, axis=1)


def shares(number_of, total, most, skew, full):
    loads = [(1 << 20) // math.isqrt(grade ** skew) + 1 for grade in range(1, number_of + 1)]
    largest = most if full else min(most, max(-(-total // number_of), total * loads[0] // sum(loads)))
    least = 1 if total - largest >= number_of - 1 else 0
    given, spare = [largest] + [least] * (number_of - 1), total - largest - least * (number_of - 1)
    while spare > 0:
        candidates = [i for i in range(1, number_of) if given[i] < largest] or [i for i in range(1, number_of) if given[i] < most]
        mass, left = sum([loads[i] for i in candidates]), spare
        for i in candidates:
            more = min(most - given[i], max(1, left * loads[i] // mass), spare)
            given[i] = given[i] + more
            spare = spare - more
    return np.array(given)


def scatter_about(key, dims, scale, limit, pieces=(), kind=jnp.bfloat16):
    factor_of = levels(key, dims, pieces, -0.22, 0.18) if pieces else 1.0
    values = jax.random.normal(key, dims, jnp.float32) * scale * factor_of
    return jnp.minimum(jnp.maximum(values, -limit), limit).astype(kind)


def setup_inputs(seed: int = 0) -> dict:
    streams_of = jax.random.split(jax.random.key(seed), 14)
    out_gate = scatter_about(streams_of[0], (TOKENS_A, D), 1.0, 6.0, ((0, 256),))
    in_gate = scatter_about(streams_of[1], (TOKENS_A, D), 1.0, 6.0, ((0, 256),))
    values = scatter_about(streams_of[2], (TOKENS_A, D), 1.0, 6.0, ((0, 256),))
    conv_taps = scatter_about(streams_of[3], (CONV, D), 0.6, 4.0, (), jnp.float32)
    out_weight = scatter_about(streams_of[4], (D, D), D ** -0.5, 0.125, ((1, 8),))
    expert_input = scatter_about(streams_of[5], (TOKENS_B, D), 1.0, 6.0, ((0, 256),))
    norm_gain = jnp.clip(1.0 + 0.18 * jax.random.normal(streams_of[6], (D,), jnp.float32), 0.1, 1.9)
    expert_ids_keys = jax.random.split(jax.random.fold_in(streams_of[7], 1), TOKENS_B // TOK_B)
    expert_ids_turns = jax.random.permutation(jax.random.fold_in(streams_of[7], 3), TOKENS_B // TOK_B)
    expert_ids = jax.vmap(lambda own, number: shared_out(jax.random.fold_in(streams_of[7], 2), own, number, TOK_B, EXPERTS, TOP, CAP, 2))(expert_ids_keys, expert_ids_turns).reshape((TOKENS_B, TOP))
    route_logits = scatter_about(streams_of[8], (TOKENS_B, TOP), 1.5, 8.0, ((0, 256),), jnp.float32)
    group_share = jnp.clip(0.3 + 0.7 * jax.random.uniform(streams_of[9], (TOKENS_B,), jnp.float32) ** levels(streams_of[9], (TOKENS_B,), ((0, 256),), -0.2, 0.2), 0.3, 1.0)
    gate_weight = scatter_about(streams_of[10], (EXPERTS, D, F), D ** -0.5, 0.125, ((0, 32),))
    up_weight = scatter_about(streams_of[11], (EXPERTS, D, F), D ** -0.5, 0.125, ((0, 32),))
    down_weight = scatter_about(streams_of[12], (EXPERTS, F, D), F ** -0.5, 0.25, ((0, 32),))
    return {"out_gate": out_gate, "in_gate": in_gate, "values": values, "conv_taps": conv_taps, "out_weight": out_weight, "expert_input": expert_input, "norm_gain": norm_gain, "expert_ids": expert_ids, "route_logits": route_logits, "group_share": group_share, "gate_weight": gate_weight, "up_weight": up_weight, "down_weight": down_weight}


norm_eps = 1e-05

def reference(out_gate, in_gate, values, conv_taps, out_weight, expert_input, norm_gain, expert_ids, route_logits, group_share, gate_weight, up_weight, down_weight):
    gated = (in_gate.astype(jnp.float32) * values.astype(jnp.float32)).astype(jnp.bfloat16)
    per_seq = gated.reshape(SEQS, -1, D).astype(jnp.float32)
    length = per_seq.shape[1]
    padded = jnp.pad(per_seq, ((0, 0), (CONV - 1, 0), (0, 0)))
    filtered = jnp.zeros_like(per_seq)
    for index in range(CONV):
        filtered = filtered + padded[:, index:index + length] * conv_taps[index]
    mixed_rows = (out_gate.astype(jnp.float32) * filtered.reshape(-1, D)).astype(jnp.bfloat16)
    mixer_out = jnp.dot(mixed_rows, out_weight, preferred_element_type=jnp.float32).astype(jnp.bfloat16)
    inputs = expert_input.astype(jnp.float32)
    scale = lax.rsqrt(lax.optimization_barrier(jnp.mean(inputs * inputs, axis=-1, keepdims=True)) + norm_eps)
    normed = (inputs * scale * norm_gain).astype(jnp.bfloat16)
    total = TOKENS_B * TOP
    flat_ids = expert_ids.reshape(-1).astype(jnp.int32)
    order = jnp.argsort(flat_ids, stable=True).astype(jnp.int32)
    counts = jax.ops.segment_sum(jnp.ones((total,), jnp.int32), flat_ids, EXPERTS).astype(jnp.int32)
    starts = (jnp.cumsum(counts) - counts).astype(jnp.int32)
    bound = N_EP * N_TP * CAP
    steps_in = jnp.arange(bound, dtype=jnp.int32)

    def per_expert(stored, expert):
        places = starts[expert] + steps_in
        valid = steps_in < counts[expert]
        entry = order[jnp.minimum(places, total - 1)]
        rows = normed[entry // TOP]
        gate = jnp.dot(rows, gate_weight[expert], preferred_element_type=jnp.float32)
        upper = jnp.dot(rows, up_weight[expert], preferred_element_type=jnp.float32)
        hidden = (jax.nn.silu(gate) * upper).astype(jnp.bfloat16)
        result = jnp.dot(hidden, down_weight[expert], preferred_element_type=jnp.float32).astype(jnp.bfloat16)
        target = jnp.where(valid, entry, total).astype(jnp.int32)
        return (stored.at[target].set(result, mode='drop'), None)
    stored = jnp.zeros((total, D), jnp.bfloat16)
    stored, _ = lax.scan(per_expert, stored, jnp.arange(EXPERTS, dtype=jnp.int32))
    expert_out = stored.reshape(TOKENS_B, TOP, D).astype(jnp.float32)
    margin = route_logits[:, 0] - route_logits[:, 1]
    route_weight = group_share[:, None] * jnp.stack([jax.nn.sigmoid(margin), jax.nn.sigmoid(-margin)], axis=1)
    expert_mix = lax.optimization_barrier(jnp.sum(expert_out * route_weight[:, :, None], axis=1)).astype(jnp.bfloat16)
    return (mixer_out, expert_mix)
```

```python
import functools

import jax
import jax.numpy as jnp
from jax import lax
from jax.experimental import pallas as pl
from jax.experimental.pallas import tpu as pltpu
from jax.sharding import PartitionSpec as P

SEQS = 1
norm_eps = 1e-05
MESH = pl.DeviceIdType.MESH

NX, NY, NZ, NC = 4, 4, 8, 2
PLANE = NX * NY * NC
COLS = 512
GU_ROWS = 64
D_ROWS = 128


def moe_kernel(
    x_ref,
    gain_ref,
    ids_row_ref,
    ids_col_ref,
    logits_ref,
    share_ref,
    gate_hbm,
    up_hbm,
    down_hbm,
    out_ref,
    normed,
    combine,
    outgoing,
    rows,
    gu,
    down,
    acc,
    hidden,
    results,
    returned,
    w_sem,
    w_send,
    x_recv,
    x_send,
    r_recv,
    r_send,
):
    tokens, width = x_ref.shape
    cap = outgoing.shape[1] // PLANE
    chunks = width // COLS
    inner = hidden.shape[1]
    gu_hops = width // GU_ROWS
    d_hops = inner // D_ROWS

    ep, tp = lax.axis_index("ep"), lax.axis_index("tp")
    z, x = lax.div(ep, NX), lax.rem(ep, NX)
    y, c = lax.div(tp, NC), lax.rem(tp, NC)
    me = (c * NY + y) * NX + x
    ahead = lax.rem(z + 1, NZ) * NX + x
    behind = lax.rem(z + NZ - 1, NZ) * NX + x
    dist = lax.rem(z + NZ - (y + NY * c), NZ)
    is_home = dist == 0
    send_up = dist <= NZ // 2 - 1
    send_down = jnp.logical_or(dist == 0, dist >= NZ // 2 + 2)

    def peer(step):
        px = lax.rem(x + lax.rem(step, NX), NX)
        py = lax.rem(y + lax.rem(lax.div(step, NX), NY), NY)
        pc = lax.rem(c + lax.div(step, NX * NY), NC)
        return (pc * NY + py) * NX + px, z * NX + px, py * NC + pc

    def gu_at(i):
        return gu.at[pl.ds(pl.multiple_of(i * GU_ROWS, GU_ROWS), GU_ROWS), :]

    def down_at(j, i):
        return down.at[j, pl.ds(pl.multiple_of(i * D_ROWS, D_ROWS), D_ROWS), :]

    @pl.when(is_home)
    def _():
        def load_gu(i, _):
            at = pl.ds(pl.multiple_of(i * GU_ROWS, GU_ROWS), GU_ROWS)
            pltpu.make_async_copy(gate_hbm.at[0, at, :], gu.at[at, pl.ds(0, inner)], w_sem.at[i]).start()
            pltpu.make_async_copy(up_hbm.at[0, at, :], gu.at[at, pl.ds(inner, inner)], w_sem.at[i]).start()
            return 0

        lax.fori_loop(0, gu_hops, load_gu, 0)
        for j in range(chunks):
            for i in range(d_hops):
                pltpu.make_async_copy(
                    down_hbm.at[0, pl.ds(i * D_ROWS, D_ROWS), pl.ds(j * COLS, COLS)],
                    down.at[j, pl.ds(i * D_ROWS, D_ROWS), :],
                    w_sem.at[gu_hops + j * d_hops + i],
                ).start()

    barrier = pltpu.get_barrier_semaphore()

    def greet(step, _):
        _, pep, ptp = peer(step)
        pl.semaphore_signal(barrier, inc=1, device_id=(pep, ptp), device_id_type=MESH)
        return 0

    lax.fori_loop(1, PLANE, greet, 0)
    for other in (ahead, behind):
        pl.semaphore_signal(barrier, inc=1, device_id=(other, tp), device_id_type=MESH)

    xf = x_ref[...].astype(jnp.float32)
    scale = lax.rsqrt(jnp.mean(xf * xf, axis=-1, keepdims=True) + norm_eps)
    normed[...] = (xf * scale * gain_ref[...]).astype(jnp.bfloat16)

    expert_sub = lax.broadcasted_iota(jnp.int32, (PLANE, tokens), 0)
    t_sub = lax.broadcasted_iota(jnp.int32, (tokens, tokens), 0)
    t_lane = lax.broadcasted_iota(jnp.int32, (tokens, tokens), 1)
    earlier_cols = jnp.where(t_sub < t_lane, 1.0, 0.0).astype(jnp.bfloat16)
    earlier_rows = jnp.where(t_lane < t_sub, 1.0, 0.0).astype(jnp.bfloat16)

    id0, id1 = ids_row_ref[0:1, :], ids_row_ref[1:2, :]
    hot0 = jnp.where(expert_sub == id0, 1.0, 0.0)
    hot1 = jnp.where(expert_sub == id1, 1.0, 0.0)
    before0 = jnp.dot(hot0.astype(jnp.bfloat16), earlier_cols, preferred_element_type=jnp.float32)
    before1 = jnp.dot(hot1.astype(jnp.bfloat16), earlier_cols, preferred_element_type=jnp.float32)
    before1 = before1 + jnp.sum(hot0, axis=1, keepdims=True)
    place0 = id0 * cap + jnp.sum(hot0 * before0, axis=0, keepdims=True).astype(jnp.int32)
    place1 = id1 * cap + jnp.sum(hot1 * before1, axis=0, keepdims=True).astype(jnp.int32)

    def spread(block):
        row = block * 256 + lax.broadcasted_iota(jnp.int32, (256, tokens), 0)
        hit = jnp.logical_or(row == place0, row == place1)
        return jnp.where(hit, 1.0, 0.0).astype(jnp.bfloat16)

    def fill(k):
        for block in range(PLANE * cap // 256):
            outgoing[k, block * 256 : (block + 1) * 256, :] = jnp.dot(
                spread(block), normed[:, k * COLS : (k + 1) * COLS], preferred_element_type=jnp.float32
            ).astype(jnp.bfloat16)

    mine = pl.ds(pl.multiple_of(me * cap, cap), cap)

    def exchange(src, dst, k, send_sem, recv_sem):
        def one(step, _):
            j, pep, ptp = peer(step)
            pltpu.make_async_remote_copy(
                src_ref=src.at[k, pl.ds(pl.multiple_of(j * cap, cap), cap), :],
                dst_ref=dst.at[k, mine, :],
                send_sem=send_sem.at[k],
                recv_sem=recv_sem.at[k],
                device_id=(pep, ptp),
                device_id_type=MESH,
            ).start()
            return 0

        lax.fori_loop(1, PLANE, one, 0)
        dst[k, mine, :] = src[k, mine, :]

    def all_of(ref, k, sem):
        span = ref.at[k, pl.ds(0, (PLANE - 1) * cap), :]
        pltpu.make_async_copy(span, span, sem.at[k]).wait()

    def relay(part, sem, which):
        pltpu.make_async_copy(part, part, sem).wait()
        for go, other, way in ((send_up, ahead, 0), (send_down, behind, 1)):

            @pl.when(go)
            def _():
                pltpu.make_async_remote_copy(
                    src_ref=part,
                    dst_ref=part,
                    send_sem=w_send.at[way, which],
                    recv_sem=sem,
                    device_id=(other, tp),
                    device_id_type=MESH,
                ).start()

    def relay_gu(k):
        per = COLS // GU_ROWS

        def one(i, _):
            relay(gu_at(i), w_sem.at[i], 0)
            return 0

        lax.fori_loop(k * per, (k + 1) * per, one, 0)

    def relay_down(j):
        def one(i, _):
            relay(down_at(j, i), w_sem.at[gu_hops + j * d_hops + i], 1)
            return 0

        lax.fori_loop(0, d_hops, one, 0)

    def project(k):
        def one(n, _):
            at = pl.ds(pl.multiple_of(n * 256, 256), 256)
            part = jnp.dot(
                rows[k, :, :], gu[k * COLS : (k + 1) * COLS, at], preferred_element_type=jnp.float32
            )
            if k == 0:
                acc[:, at] = part
            else:
                acc[:, at] += part
            return 0

        lax.fori_loop(0, 2 * inner // 256, one, 0)

    def activate():
        def one(b, _):
            at = pl.ds(pl.multiple_of(b * 128, 128), 128)
            g, u = acc[at, 0:inner], acc[at, inner:]
            hidden[at, :] = (g * jax.nn.sigmoid(g) * u).astype(jnp.bfloat16)
            return 0

        lax.fori_loop(0, PLANE * cap // 128, one, 0)

    def produce(j):
        def one(n, _):
            at = pl.ds(pl.multiple_of(n * 256, 256), 256)
            results[j, :, at] = jnp.dot(
                hidden[...], down[j, :, at], preferred_element_type=jnp.float32
            ).astype(jnp.bfloat16)
            return 0

        lax.fori_loop(0, COLS // 256, one, 0)

    fill(0)
    pl.semaphore_wait(barrier, PLANE - 1 + 2)
    exchange(outgoing, rows, 0, x_send, x_recv)
    for k in range(1, chunks):
        fill(k)
        exchange(outgoing, rows, k, x_send, x_recv)

    expert_lane = lax.broadcasted_iota(jnp.int32, (tokens, 128), 1)
    cid0, cid1 = ids_col_ref[:, 0:1], ids_col_ref[:, 1:2]
    chot0 = jnp.where(expert_lane == cid0, 1.0, 0.0)
    chot1 = jnp.where(expert_lane == cid1, 1.0, 0.0)
    cbefore0 = jnp.dot(earlier_rows, chot0.astype(jnp.bfloat16), preferred_element_type=jnp.float32)
    cbefore1 = jnp.dot(earlier_rows, chot1.astype(jnp.bfloat16), preferred_element_type=jnp.float32)
    cbefore1 = cbefore1 + jnp.sum(chot0, axis=0, keepdims=True)
    cplace0 = cid0 * cap + jnp.sum(chot0 * cbefore0, axis=1, keepdims=True).astype(jnp.int32)
    cplace1 = cid1 * cap + jnp.sum(chot1 * cbefore1, axis=1, keepdims=True).astype(jnp.int32)
    margin = logits_ref[:, 0:1] - logits_ref[:, 1:2]
    weight0 = share_ref[...] * jax.nn.sigmoid(margin)
    weight1 = share_ref[...] * jax.nn.sigmoid(-margin)
    for block in range(PLANE * cap // 256):
        column = block * 256 + lax.broadcasted_iota(jnp.int32, (tokens, 256), 1)
        weight = jnp.where(column == cplace0, weight0, 0.0) + jnp.where(column == cplace1, weight1, 0.0)
        coarse = weight.astype(jnp.bfloat16)
        combine[0, :, block * 256 : (block + 1) * 256] = coarse
        combine[1, :, block * 256 : (block + 1) * 256] = (weight - coarse.astype(jnp.float32)).astype(jnp.bfloat16)

    relay_gu(0)
    for k in range(chunks):
        if k + 1 < chunks:
            relay_gu(k + 1)
        all_of(rows, k, x_recv)
        project(k)
    activate()
    for j in range(chunks):
        relay_down(j)
        produce(j)
        exchange(results, returned, j, r_send, r_recv)
    for j in range(chunks):
        all_of(returned, j, r_recv)
        mix = jnp.dot(combine[0], returned[j], preferred_element_type=jnp.float32)
        mix = mix + jnp.dot(combine[1], returned[j], preferred_element_type=jnp.float32)
        out_ref[:, j * COLS : (j + 1) * COLS] = mix.astype(jnp.bfloat16)

    for k in range(chunks):
        all_of(outgoing, k, x_send)
        all_of(results, k, r_send)
    for go, way in ((send_up, 0), (send_down, 1)):

        @pl.when(go)
        def _():
            pltpu.make_async_copy(gu, gu, w_send.at[way, 0]).wait()
            pltpu.make_async_copy(down, down, w_send.at[way, 1]).wait()


def moe(expert_input, norm_gain, expert_ids, route_logits, group_share, gate_weight, up_weight, down_weight):
    tokens, width = expert_input.shape
    inner = gate_weight.shape[2]
    cap = 2 * tokens * expert_ids.shape[1] // PLANE
    chunks = width // COLS
    slots = PLANE * cap
    hops = width // GU_ROWS + chunks * (inner // D_ROWS)
    vmem = pl.BlockSpec(memory_space=pltpu.VMEM)
    hbm = pl.BlockSpec(memory_space=pl.ANY)
    bf = jnp.bfloat16
    return pl.pallas_call(
        moe_kernel,
        out_shape=jax.ShapeDtypeStruct((tokens, width), bf),
        in_specs=[vmem] * 6 + [hbm] * 3,
        out_specs=vmem,
        scratch_shapes=[
            pltpu.VMEM((tokens, width), bf),
            pltpu.VMEM((2, tokens, slots), bf),
            pltpu.VMEM((chunks, slots, COLS), bf),
            pltpu.VMEM((chunks, slots, COLS), bf),
            pltpu.VMEM((width, 2 * inner), bf),
            pltpu.VMEM((chunks, inner, COLS), bf),
            pltpu.VMEM((slots, 2 * inner), jnp.float32),
            pltpu.VMEM((slots, inner), bf),
            pltpu.VMEM((chunks, slots, COLS), bf),
            pltpu.VMEM((chunks, slots, COLS), bf),
            pltpu.SemaphoreType.DMA((hops,)),
            pltpu.SemaphoreType.DMA((2, 2)),
            pltpu.SemaphoreType.DMA((chunks,)),
            pltpu.SemaphoreType.DMA((chunks,)),
            pltpu.SemaphoreType.DMA((chunks,)),
            pltpu.SemaphoreType.DMA((chunks,)),
        ],
        compiler_params=pltpu.CompilerParams(
            collective_id=0, has_side_effects=True, vmem_limit_bytes=60 * 1024 * 1024
        ),
        cost_estimate=pl.CostEstimate(flops=100_000_000_000, bytes_accessed=10_000_000, transcendentals=1_000_000),
        name="moe",
    )(
        expert_input,
        norm_gain[None, :],
        expert_ids.T,
        expert_ids,
        route_logits,
        group_share[:, None],
        gate_weight,
        up_weight,
        down_weight,
    )


def passed_along(value, axis, by):
    length = lax.axis_size(axis)
    pairs = [(i, i + by) for i in range(length) if 0 <= i + by < length]
    return lax.ppermute(value, axis, pairs)


def mixer(out_gate, in_gate, values, conv_taps, out_weight):
    rows_mix, width = out_gate.shape
    extent = conv_taps.shape[0] - 1
    gated = (in_gate.astype(jnp.float32) * values.astype(jnp.float32)).astype(jnp.bfloat16)
    before = passed_along(gated[rows_mix - extent :], ("ep", "tp"), 1)
    extended = jnp.concatenate([before, gated], axis=0)
    devices = lax.axis_size("ep") * lax.axis_size("tp")
    seq_len = devices * rows_mix // SEQS
    position = lax.axis_index(("ep", "tp")) * rows_mix + jnp.arange(rows_mix, dtype=jnp.int32)
    offset = position % seq_len
    filtered = jnp.zeros((rows_mix, width), jnp.float32)
    for delays in range(extent + 1):
        lagged = extended[extent - delays : extent - delays + rows_mix].astype(jnp.float32)
        if delays > 0:
            lagged = jnp.where((offset >= delays)[:, None], lagged, 0.0)
        filtered = filtered + conv_taps[extent - delays] * lagged
    mixed_rows = (out_gate.astype(jnp.float32) * filtered).astype(jnp.bfloat16)
    return jnp.dot(
        mixed_rows,
        lax.all_gather(out_weight, "tp", axis=1, tiled=True),
        preferred_element_type=jnp.float32,
    ).astype(jnp.bfloat16)


def local(
    out_gate,
    in_gate,
    values,
    conv_taps,
    out_weight,
    expert_input,
    norm_gain,
    expert_ids,
    route_logits,
    group_share,
    gate_weight,
    up_weight,
    down_weight,
):
    mixer_out = mixer(out_gate, in_gate, values, conv_taps, out_weight)
    expert_mix = moe(
        expert_input, norm_gain, expert_ids, route_logits, group_share, gate_weight, up_weight, down_weight
    )
    return (mixer_out, expert_mix)


def solution(mesh):
    return jax.shard_map(
        local,
        mesh=mesh,
        in_specs=(
            P(("ep", "tp"), None),
            P(("ep", "tp"), None),
            P(("ep", "tp"), None),
            P(),
            P(None, "tp"),
            P(("ep", "tp"), None),
            P(),
            P(("ep", "tp"), None),
            P(("ep", "tp"), None),
            P(("ep", "tp")),
            P("ep", None, None),
            P("ep", None, None),
            P("ep", None, None),
        ),
        out_specs=(P(("ep", "tp"), None), P(("ep", "tp"), None)),
        check_vma=False,
    )
```

```python
import functools

import jax
import jax.numpy as jnp
from jax import lax
from jax.experimental import pallas as pl
from jax.experimental.pallas import tpu as pltpu
from jax.sharding import PartitionSpec as P

SEQS = 1
norm_eps = 1e-05
MESH = pl.DeviceIdType.MESH

NX, NY, NZ, NC = 4, 4, 8, 2
PLANE = NX * NY * NC
COLS = 512
GU_ROWS = 64
D_ROWS = 128


def step_kernel(
    x_ref,
    gain_ref,
    ids_ref,
    logits_ref,
    share_ref,
    taps_ref,
    og_hbm,
    ig_hbm,
    val_hbm,
    block_hbm,
    gate_hbm,
    up_hbm,
    down_hbm,
    mixer_ref,
    out_ref,
    normed,
    combine,
    outgoing,
    rows,
    gu,
    down,
    acc,
    hidden,
    results,
    returned,
    og,
    ig,
    val,
    gated,
    tail,
    halo,
    mixed,
    project_w,
    mixer_acc,
    w_sem,
    w_send,
    x_recv,
    x_send,
    r_recv,
    r_send,
    in_sem,
    halo_sem,
    share_sem,
    ring_recv,
    ring_send,
    pair_recv,
    pair_send,
):
    tokens, width = x_ref.shape
    cap = outgoing.shape[1] // PLANE
    chunks = width // COLS
    inner = hidden.shape[1]
    gu_hops = width // GU_ROWS
    d_hops = inner // D_ROWS
    rows_mix = og.shape[0]
    part = width // NZ

    ep, tp = lax.axis_index("ep"), lax.axis_index("tp")
    z, x = lax.div(ep, NX), lax.rem(ep, NX)
    y, c = lax.div(tp, NC), lax.rem(tp, NC)
    me = (c * NY + y) * NX + x
    ahead = lax.rem(z + 1, NZ) * NX + x
    behind = lax.rem(z + NZ - 1, NZ) * NX + x
    dist = lax.rem(z + NZ - (y + NY * c), NZ)
    is_home = dist == 0
    pair = y * NC + 1 - c
    n_ep, n_tp = NZ * NX, NY * NC
    flat = ep * n_tp + tp
    later = lax.rem(flat + 1, n_ep * n_tp)
    sooner = lax.rem(flat + n_ep * n_tp - 1, n_ep * n_tp)

    def peer(step):
        px = lax.rem(x + lax.rem(step, NX), NX)
        py = lax.rem(y + lax.rem(lax.div(step, NX), NY), NY)
        pc = lax.rem(c + lax.div(step, NX * NY), NC)
        return (pc * NY + py) * NX + px, z * NX + px, py * NC + pc

    def send(src, dst, send_sem, recv_sem, to):
        pltpu.make_async_remote_copy(
            src_ref=src,
            dst_ref=dst,
            send_sem=send_sem,
            recv_sem=recv_sem,
            device_id=to,
            device_id_type=MESH,
        ).start()

    def settle(ref, sem):
        pltpu.make_async_copy(ref, ref, sem).wait()

    def gu_at(i):
        return gu.at[pl.ds(pl.multiple_of(i * GU_ROWS, GU_ROWS), GU_ROWS), :]

    def down_at(j, i):
        return down.at[j, pl.ds(pl.multiple_of(i * D_ROWS, D_ROWS), D_ROWS), :]

    @pl.when(is_home)
    def _():
        def load_gu(i, _):
            at = pl.ds(pl.multiple_of(i * GU_ROWS, GU_ROWS), GU_ROWS)
            pltpu.make_async_copy(gate_hbm.at[0, at, :], gu.at[at, pl.ds(0, inner)], w_sem.at[i]).start()
            pltpu.make_async_copy(up_hbm.at[0, at, :], gu.at[at, pl.ds(inner, inner)], w_sem.at[i]).start()
            return 0

        lax.fori_loop(0, gu_hops, load_gu, 0)
        for j in range(chunks):
            for i in range(d_hops):
                pltpu.make_async_copy(
                    down_hbm.at[0, pl.ds(i * D_ROWS, D_ROWS), pl.ds(j * COLS, COLS)],
                    down.at[j, pl.ds(i * D_ROWS, D_ROWS), :],
                    w_sem.at[gu_hops + j * d_hops + i],
                ).start()

    loads = [
        pltpu.make_async_copy(ig_hbm, ig, in_sem.at[0]),
        pltpu.make_async_copy(val_hbm, val, in_sem.at[1]),
        pltpu.make_async_copy(og_hbm, og, in_sem.at[2]),
        pltpu.make_async_copy(block_hbm, project_w.at[tp], in_sem.at[3]),
    ]
    for load in loads:
        load.start()

    barrier = pltpu.get_barrier_semaphore()

    def greet(step, _):
        _, pep, ptp = peer(step)
        pl.semaphore_signal(barrier, inc=1, device_id=(pep, ptp), device_id_type=MESH)
        return 0

    lax.fori_loop(1, PLANE, greet, 0)
    for other in (ahead, behind):
        pl.semaphore_signal(barrier, inc=1, device_id=(other, tp), device_id_type=MESH)
    for other in (later, sooner):
        pl.semaphore_signal(
            barrier, inc=1, device_id=(lax.div(other, n_tp), lax.rem(other, n_tp)), device_id_type=MESH
        )

    xf = x_ref[...].astype(jnp.float32)
    scale = lax.rsqrt(jnp.mean(xf * xf, axis=-1, keepdims=True) + norm_eps)
    normed[...] = (xf * scale * gain_ref[...]).astype(jnp.bfloat16)

    loads[0].wait()
    loads[1].wait()
    product = (ig[...].astype(jnp.float32) * val[...].astype(jnp.float32)).astype(jnp.bfloat16)
    tail[...] = product[rows_mix - 16 :, :]
    gated[8:, :] = product.astype(jnp.float32)

    expert_sub = lax.broadcasted_iota(jnp.int32, (PLANE, tokens), 0)
    t_sub = lax.broadcasted_iota(jnp.int32, (tokens, tokens), 0)
    t_lane = lax.broadcasted_iota(jnp.int32, (tokens, tokens), 1)
    earlier = jnp.where(t_sub < t_lane, 1.0, 0.0).astype(jnp.bfloat16)
    id0, id1 = ids_ref[0:1, :], ids_ref[1:2, :]
    hot0 = jnp.where(expert_sub == id0, 1.0, 0.0)
    hot1 = jnp.where(expert_sub == id1, 1.0, 0.0)
    before0 = jnp.dot(hot0.astype(jnp.bfloat16), earlier, preferred_element_type=jnp.float32)
    before1 = jnp.dot(hot1.astype(jnp.bfloat16), earlier, preferred_element_type=jnp.float32)
    before1 = before1 + jnp.sum(hot0, axis=1, keepdims=True)
    slot0 = jnp.sum(hot0 * before0, axis=0, keepdims=True)
    slot1 = jnp.sum(hot1 * before1, axis=0, keepdims=True)
    place0 = id0 * cap + slot0.astype(jnp.int32)
    place1 = id1 * cap + slot1.astype(jnp.int32)

    def fill(k):
        for block in range(PLANE * cap // 256):
            row = block * 256 + lax.broadcasted_iota(jnp.int32, (256, tokens), 0)
            hit = jnp.logical_or(row == place0, row == place1)
            outgoing[k, block * 256 : (block + 1) * 256, :] = jnp.dot(
                jnp.where(hit, 1.0, 0.0).astype(jnp.bfloat16),
                normed[:, k * COLS : (k + 1) * COLS],
                preferred_element_type=jnp.float32,
            ).astype(jnp.bfloat16)

    mine = pl.ds(pl.multiple_of(me * cap, cap), cap)

    def exchange(src, dst, k, send_sem, recv_sem):
        dst[k, mine, :] = src[k, mine, :]

        def one(step, _):
            j, pep, ptp = peer(step)
            send(
                src.at[k, pl.ds(pl.multiple_of(j * cap, cap), cap), :],
                dst.at[k, mine, :],
                send_sem.at[k],
                recv_sem.at[k],
                (pep, ptp),
            )
            return 0

        lax.fori_loop(1, PLANE, one, 0)

    def all_of(ref, k, sem):
        settle(ref.at[k, pl.ds(0, (PLANE - 1) * cap), :], sem.at[k])

    half = NZ // 2

    def pass_on(piece, i, sem, which):
        up = jnp.logical_or(dist < half - 1, jnp.logical_and(dist == half - 1, lax.rem(i, 2) == 0))
        back = jnp.logical_or(
            jnp.logical_or(dist == 0, dist > half + 1), jnp.logical_and(dist == half + 1, lax.rem(i, 2) == 1)
        )
        for go, other, way in ((up, ahead, 0), (back, behind, 1)):

            @pl.when(go)
            def _():
                send(piece, piece, w_send.at[way, which], sem, (other, tp))

    def relay_gu(start, stop):
        def one(i, _):
            settle(gu_at(i), w_sem.at[i])
            pass_on(gu_at(i), i, w_sem.at[i], 0)
            return 0

        lax.fori_loop(start, stop, one, 0)

    def relay_down(j):
        def one(i, _):
            sem = w_sem.at[gu_hops + j * d_hops + i]
            settle(down_at(j, i), sem)
            pass_on(down_at(j, i), i, sem, 1)
            return 0

        lax.fori_loop(0, d_hops, one, 0)

    def project(k):
        def one(n, _):
            at = pl.ds(pl.multiple_of(n * 256, 256), 256)
            product = jnp.dot(rows[k, :, :], gu[k * COLS : (k + 1) * COLS, at], preferred_element_type=jnp.float32)
            if k == 0:
                acc[:, at] = product
            else:
                acc[:, at] += product
            return 0

        lax.fori_loop(0, 2 * inner // 256, one, 0)

    def activate():
        def one(b, _):
            at = pl.ds(pl.multiple_of(b * 128, 128), 128)
            g, u = acc[at, 0:inner], acc[at, inner:]
            hidden[at, :] = (g * jax.nn.sigmoid(g) * u).astype(jnp.bfloat16)
            return 0

        lax.fori_loop(0, PLANE * cap // 128, one, 0)

    def produce(j):
        def one(n, _):
            at = pl.ds(pl.multiple_of(n * 256, 256), 256)
            results[j, :, at] = jnp.dot(hidden[...], down[j, :, at], preferred_element_type=jnp.float32).astype(
                jnp.bfloat16
            )
            return 0

        lax.fori_loop(0, COLS // 256, one, 0)

    def mix(j):
        all_of(returned, j, r_recv)
        total = jnp.dot(combine[0], returned[j], preferred_element_type=jnp.float32)
        total = total + jnp.dot(combine[1], returned[j], preferred_element_type=jnp.float32)
        out_ref[:, j * COLS : (j + 1) * COLS] = total.astype(jnp.bfloat16)

    def near(i):
        return lax.rem(y + 1 + i, NY) * NC + c

    def share_of(b, q):
        return project_w.at[b, pl.ds(pl.multiple_of(q * part, part), part), :]

    others = NY - 1
    three = project_w.at[0, pl.ds(0, others * part), :]

    def to_pair(q):
        def one(i, _):
            send(share_of(near(i), q), share_of(near(i), q), pair_send.at[q], pair_recv.at[q], (ep, pair))
            return 0

        lax.fori_loop(0, others, one, 0)

    def goes_up(i):
        return jnp.logical_or(i == 0, jnp.logical_and(i == 2, c == 0))

    def ring_send_piece(q, way, m, i):
        other = ahead if way == 0 else behind
        piece = share_of(near(i), q)
        send(piece, piece, ring_send.at[way, m, i], ring_recv.at[way, m, i], (other, tp))

    def ring_start():
        def one(i, _):
            for way in (0, 1):
                ring_send_piece(z, way, 0, i)
            return 0

        lax.fori_loop(0, others, one, 0)

    def ring_step(k):
        for way in (0, 1):
            q = lax.rem(z + NZ - k, NZ) if way == 0 else lax.rem(z + k, NZ)

            def one(i, _):
                settle(share_of(near(i), q), ring_recv.at[way, k - 1, i])
                if k < half - 1:
                    ring_send_piece(q, way, k, i)
                else:

                    @pl.when(goes_up(i) if way == 0 else jnp.logical_not(goes_up(i)))
                    def _():
                        ring_send_piece(q, way, k, i)

                return 0

            lax.fori_loop(0, others, one, 0)
            to_pair(q)

    def ring_last():
        q = lax.rem(z + half, NZ)

        def one(i, _):
            @pl.when(goes_up(i))
            def _():
                settle(share_of(near(i), q), ring_recv.at[0, half - 1, i])

            @pl.when(jnp.logical_not(goes_up(i)))
            def _():
                settle(share_of(near(i), q), ring_recv.at[1, half - 1, i])

            return 0

        lax.fori_loop(0, others, one, 0)
        to_pair(q)

    def mixer_part(q, first=False):
        settle(three, pair_recv.at[q])
        at = pl.ds(pl.multiple_of(q * part, part), part)

        def one(b, _):
            to = pl.ds(pl.multiple_of(b * block_cols, block_cols), block_cols)
            product = jnp.dot(mixed[:, at], project_w[b, at, :], preferred_element_type=jnp.float32)
            if first:
                mixer_acc[:, to] = product
            else:
                mixer_acc[:, to] += product
            return 0

        lax.fori_loop(0, n_tp, one, 0)

    block_cols = project_w.shape[2]

    pl.semaphore_wait(barrier, PLANE - 1 + 4)
    send(tail, halo, halo_sem.at[0], halo_sem.at[1], (lax.div(later, n_tp), lax.rem(later, n_tp)))

    @pl.when(is_home)
    def _():
        relay_gu(0, 8)

    fill(0)
    exchange(outgoing, rows, 0, x_send, x_recv)
    fill(1)
    exchange(outgoing, rows, 1, x_send, x_recv)

    @pl.when(is_home)
    def _():
        relay_gu(8, gu_hops)
        for j in range(chunks):
            relay_down(j)

    away = jnp.logical_not(is_home)

    @pl.when(away)
    def _():
        relay_gu(0, 4)

    fill(2)
    exchange(outgoing, rows, 2, x_send, x_recv)

    @pl.when(away)
    def _():
        relay_gu(4, 8)

    fill(3)
    exchange(outgoing, rows, 3, x_send, x_recv)

    loads[3].wait()

    def give(i, _):
        piece = share_of(tp, z)
        send(piece, piece, share_sem.at[0], share_sem.at[1], (ep, near(i)))
        return 0

    lax.fori_loop(0, others, give, 0)
    send(project_w.at[tp], project_w.at[tp], pair_send.at[NZ], pair_recv.at[NZ], (ep, pair))

    @pl.when(away)
    def _():
        relay_gu(8, 12)

    margin = logits_ref[0:1, :] - logits_ref[1:2, :]
    weight0 = share_ref[...] * jax.nn.sigmoid(margin)
    weight1 = share_ref[...] * jax.nn.sigmoid(-margin)
    lane_rows = jnp.concatenate(
        [
            place0.astype(jnp.float32),
            place1.astype(jnp.float32),
            weight0,
            weight1,
            jnp.zeros((124, tokens), jnp.float32),
        ],
        axis=0,
    )
    turned = lane_rows.T
    cplace0, cplace1 = turned[:, 0:1].astype(jnp.int32), turned[:, 1:2].astype(jnp.int32)
    cweight0, cweight1 = turned[:, 2:3], turned[:, 3:4]
    for block in range(PLANE * cap // 256):
        column = block * 256 + lax.broadcasted_iota(jnp.int32, (tokens, 256), 1)
        weight = jnp.where(column == cplace0, cweight0, 0.0) + jnp.where(column == cplace1, cweight1, 0.0)
        coarse = weight.astype(jnp.bfloat16)
        combine[0, :, block * 256 : (block + 1) * 256] = coarse
        combine[1, :, block * 256 : (block + 1) * 256] = (weight - coarse.astype(jnp.float32)).astype(jnp.bfloat16)

    @pl.when(away)
    def _():
        relay_gu(12, 16)

    all_of(rows, 0, x_recv)
    project(0)

    settle(halo, halo_sem.at[1])
    loads[2].wait()
    seq_len = n_ep * n_tp * rows_mix // SEQS
    inside = lax.rem(flat * rows_mix, seq_len) != 0
    early = halo[...].astype(jnp.float32)[8:, :]
    gated[0:8, :] = jnp.where(inside, early, 0.0)

    def filter_columns(n, _):
        at = pl.ds(pl.multiple_of(n * 256, 256), 256)
        filtered = taps_ref[0:1, at] * gated[6 : 6 + rows_mix, at]
        filtered = filtered + taps_ref[1:2, at] * gated[7 : 7 + rows_mix, at]
        filtered = filtered + taps_ref[2:3, at] * gated[8 : 8 + rows_mix, at]
        mixed[:, at] = (og[:, at].astype(jnp.float32) * filtered).astype(jnp.bfloat16)
        return 0

    lax.fori_loop(0, width // 256, filter_columns, 0)

    @pl.when(away)
    def _():
        relay_gu(16, 24)

    all_of(rows, 1, x_recv)
    project(1)

    @pl.when(away)
    def _():
        relay_gu(24, 32)

    all_of(rows, 2, x_recv)
    project(2)
    all_of(rows, 3, x_recv)
    project(3)
    activate()
    for j in range(chunks):

        @pl.when(away)
        def _():
            relay_down(j)

        produce(j)
        exchange(results, returned, j, r_send, r_recv)

    settle(three, share_sem.at[1])
    ring_start()
    to_pair(z)
    settle(project_w.at[tp], pair_recv.at[NZ])
    mixer_part(z, first=True)
    ring_step(1)
    ring_step(2)
    mix(0)
    mixer_part(lax.rem(z + NZ - 1, NZ))
    mixer_part(lax.rem(z + 1, NZ))
    ring_step(3)
    mix(1)
    mixer_part(lax.rem(z + NZ - 2, NZ))
    mixer_part(lax.rem(z + 2, NZ))
    ring_last()
    mixer_part(lax.rem(z + NZ - 3, NZ))
    mixer_part(lax.rem(z + 3, NZ))
    mix(2)
    mixer_part(lax.rem(z + half, NZ))
    mixer_ref[...] = mixer_acc[...].astype(jnp.bfloat16)
    mix(3)

    for k in range(chunks):
        all_of(outgoing, k, x_send)
        all_of(results, k, r_send)
    settle(tail, halo_sem.at[0])
    settle(three, share_sem.at[0])
    settle(project_w.at[tp], pair_send.at[NZ])

    def pairs_left(q, _):
        settle(three, pair_send.at[q])
        return 0

    lax.fori_loop(0, NZ, pairs_left, 0)

    def rings_left(i, _):
        for way in (0, 1):
            for m in range(half - 1):
                settle(share_of(0, 0), ring_send.at[way, m, i])

        @pl.when(goes_up(i))
        def _():
            settle(share_of(0, 0), ring_send.at[0, half - 1, i])

        @pl.when(jnp.logical_not(goes_up(i)))
        def _():
            settle(share_of(0, 0), ring_send.at[1, half - 1, i])

        return 0

    lax.fori_loop(0, others, rings_left, 0)

    def weights_left(way, which, some):
        ref = gu if which == 0 else down
        if some:
            ref = gu.at[pl.ds(0, width // 2), :] if which == 0 else down.at[pl.ds(0, chunks // 2), :, :]
        settle(ref, w_send.at[way, which])

    for way, full, some in (
        (0, dist < half - 1, dist == half - 1),
        (1, jnp.logical_or(dist == 0, dist > half + 1), dist == half + 1),
    ):

        @pl.when(full)
        def _():
            weights_left(way, 0, False)
            weights_left(way, 1, False)

        @pl.when(some)
        def _():
            weights_left(way, 0, True)
            weights_left(way, 1, True)


def local(
    out_gate,
    in_gate,
    values,
    conv_taps,
    out_weight,
    expert_input,
    norm_gain,
    expert_ids,
    route_logits,
    group_share,
    gate_weight,
    up_weight,
    down_weight,
):
    tokens, width = expert_input.shape
    inner = gate_weight.shape[2]
    rows_mix = out_gate.shape[0]
    cap = 2 * tokens * expert_ids.shape[1] // PLANE
    chunks = width // COLS
    slots = PLANE * cap
    hops = width // GU_ROWS + chunks * (inner // D_ROWS)
    vmem = pl.BlockSpec(memory_space=pltpu.VMEM)
    hbm = pl.BlockSpec(memory_space=pl.ANY)
    bf, dma = jnp.bfloat16, pltpu.SemaphoreType.DMA
    return pl.pallas_call(
        step_kernel,
        out_shape=(
            jax.ShapeDtypeStruct((rows_mix, width), bf),
            jax.ShapeDtypeStruct((tokens, width), bf),
        ),
        in_specs=[vmem] * 6 + [hbm] * 7,
        out_specs=(vmem, vmem),
        scratch_shapes=[
            pltpu.VMEM((tokens, width), bf),
            pltpu.VMEM((2, tokens, slots), bf),
            pltpu.VMEM((chunks, slots, COLS), bf),
            pltpu.VMEM((chunks, slots, COLS), bf),
            pltpu.VMEM((width, 2 * inner), bf),
            pltpu.VMEM((chunks, inner, COLS), bf),
            pltpu.VMEM((slots, 2 * inner), jnp.float32),
            pltpu.VMEM((slots, inner), bf),
            pltpu.VMEM((chunks, slots, COLS), bf),
            pltpu.VMEM((chunks, slots, COLS), bf),
            pltpu.VMEM((rows_mix, width), bf),
            pltpu.VMEM((rows_mix, width), bf),
            pltpu.VMEM((rows_mix, width), bf),
            pltpu.VMEM((8 + rows_mix, width), jnp.float32),
            pltpu.VMEM((16, width), bf),
            pltpu.VMEM((16, width), bf),
            pltpu.VMEM((rows_mix, width), bf),
            pltpu.VMEM((NY * NC, *out_weight.shape), bf),
            pltpu.VMEM((rows_mix, width), jnp.float32),
            dma((hops,)),
            dma((2, 2)),
            dma((chunks,)),
            dma((chunks,)),
            dma((chunks,)),
            dma((chunks,)),
            dma((4,)),
            dma((2,)),
            dma((2,)),
            dma((2, NZ // 2, NY - 1)),
            dma((2, NZ // 2, NY - 1)),
            dma((NZ + 1,)),
            dma((NZ + 1,)),
        ],
        compiler_params=pltpu.CompilerParams(
            collective_id=0, has_side_effects=True, vmem_limit_bytes=63 * 1024 * 1024
        ),
        name="layer_step",
    )(
        expert_input,
        norm_gain[None, :],
        expert_ids.T,
        route_logits.T,
        group_share[None, :],
        conv_taps,
        out_gate,
        in_gate,
        values,
        out_weight,
        gate_weight,
        up_weight,
        down_weight,
    )


def solution(mesh):
    return jax.shard_map(
        local,
        mesh=mesh,
        in_specs=(
            P(("ep", "tp"), None),
            P(("ep", "tp"), None),
            P(("ep", "tp"), None),
            P(),
            P(None, "tp"),
            P(("ep", "tp"), None),
            P(),
            P(("ep", "tp"), None),
            P(("ep", "tp"), None),
            P(("ep", "tp")),
            P("ep", None, None),
            P("ep", None, None),
            P("ep", None, None),
        ),
        out_specs=(P(("ep", "tp"), None), P(("ep", "tp"), None)),
        check_vma=False,
    )
```

```python
import functools

import jax
import jax.numpy as jnp
from jax import lax
from jax.experimental import pallas as pl
from jax.experimental.pallas import tpu as pltpu
from jax.sharding import PartitionSpec as P

SEQS = 1
norm_eps = 1e-05
MESH = pl.DeviceIdType.MESH

NX, NY, NZ, NC = 4, 4, 8, 2
PLANE = NX * NY * NC
COLS = 512
GU_ROWS = 32
D_ROWS = 64
WINDOW = 6


def step_kernel(
    x_ref,
    gain_ref,
    ids_ref,
    logits_ref,
    share_ref,
    taps_ref,
    og_hbm,
    ig_hbm,
    val_hbm,
    block_hbm,
    gate_hbm,
    up_hbm,
    down_hbm,
    mixer_hbm,
    out_hbm,
    mixer_ref,
    out_ref,
    normed,
    combine,
    outgoing,
    rows,
    gu,
    down,
    acc,
    hidden,
    results,
    returned,
    og,
    ig,
    val,
    gated,
    tail,
    halo,
    mixed,
    project_w,
    mixer_acc,
    w_sem,
    w_send,
    x_recv,
    x_send,
    r_recv,
    r_send,
    in_sem,
    halo_sem,
    share_sem,
    ring_recv,
    ring_send,
    pair_recv,
    pair_send,
    along_recv,
    along_send,
    out_sem,
):
    tokens, width = x_ref.shape
    cap = outgoing.shape[1] // PLANE
    chunks = width // COLS
    inner = hidden.shape[1]
    gu_hops = width // GU_ROWS
    d_hops = inner // D_ROWS
    rows_mix = og.shape[0]
    split, plain = width // 2, width // 4
    part, wide = split // NZ, (width - split - plain) // NX

    ep, tp = lax.axis_index("ep"), lax.axis_index("tp")
    z, x = lax.div(ep, NX), lax.rem(ep, NX)
    y, c = lax.div(tp, NC), lax.rem(tp, NC)
    me = (c * NY + y) * NX + x
    ahead = lax.rem(z + 1, NZ) * NX + x
    behind = lax.rem(z + NZ - 1, NZ) * NX + x
    dist = lax.rem(z + NZ - (y + NY * c), NZ)
    is_home = dist == 0
    pair = y * NC + 1 - c
    n_ep, n_tp = NZ * NX, NY * NC
    flat = ep * n_tp + tp
    later = lax.rem(flat + 1, n_ep * n_tp)
    sooner = lax.rem(flat + n_ep * n_tp - 1, n_ep * n_tp)

    def peer(step):
        px = lax.rem(x + lax.rem(step, NX), NX)
        py = lax.rem(y + lax.rem(lax.div(step, NX), NY), NY)
        pc = lax.rem(c + lax.div(step, NX * NY), NC)
        return (pc * NY + py) * NX + px, z * NX + px, py * NC + pc

    def send(src, dst, send_sem, recv_sem, to):
        pltpu.make_async_remote_copy(
            src_ref=src,
            dst_ref=dst,
            send_sem=send_sem,
            recv_sem=recv_sem,
            device_id=to,
            device_id_type=MESH,
        ).start()

    def settle(ref, sem):
        pltpu.make_async_copy(ref, ref, sem).wait()

    def gu_at(i):
        return gu.at[pl.ds(pl.multiple_of(i * GU_ROWS, GU_ROWS), GU_ROWS), :]

    def down_at(j, i):
        return down.at[j, pl.ds(pl.multiple_of(i * D_ROWS, D_ROWS), D_ROWS), :]

    barrier = pltpu.get_barrier_semaphore()

    def greet(step, _):
        _, pep, ptp = peer(step)
        pl.semaphore_signal(barrier, inc=1, device_id=(pep, ptp), device_id_type=MESH)
        return 0

    lax.fori_loop(1, PLANE, greet, 0)
    for other in (ahead, behind):
        pl.semaphore_signal(barrier, inc=1, device_id=(other, tp), device_id_type=MESH)
    for other in (later, sooner):
        pl.semaphore_signal(
            barrier, inc=1, device_id=(lax.div(other, n_tp), lax.rem(other, n_tp)), device_id_type=MESH
        )

    @pl.when(is_home)
    def _():
        def load_gu(i, _):
            at = pl.ds(pl.multiple_of(i * GU_ROWS, GU_ROWS), GU_ROWS)
            pltpu.make_async_copy(gate_hbm.at[0, at, :], gu.at[at, pl.ds(0, inner)], w_sem.at[i]).start()
            pltpu.make_async_copy(up_hbm.at[0, at, :], gu.at[at, pl.ds(inner, inner)], w_sem.at[i]).start()
            return 0

        lax.fori_loop(0, gu_hops, load_gu, 0)
        for j in range(chunks):
            for i in range(d_hops):
                pltpu.make_async_copy(
                    down_hbm.at[0, pl.ds(i * D_ROWS, D_ROWS), pl.ds(j * COLS, COLS)],
                    down.at[j, pl.ds(i * D_ROWS, D_ROWS), :],
                    w_sem.at[gu_hops + j * d_hops + i],
                ).start()

    loads = [
        pltpu.make_async_copy(ig_hbm, ig, in_sem.at[0]),
        pltpu.make_async_copy(val_hbm, val, in_sem.at[1]),
        pltpu.make_async_copy(og_hbm, og, in_sem.at[2]),
        pltpu.make_async_copy(block_hbm, project_w.at[tp], in_sem.at[3]),
    ]
    for load in loads:
        load.start()

    xf = x_ref[...].astype(jnp.float32)
    scale = lax.rsqrt(jnp.mean(xf * xf, axis=-1, keepdims=True) + norm_eps)
    normed[...] = (xf * scale * gain_ref[...]).astype(jnp.bfloat16)

    loads[0].wait()
    loads[1].wait()
    product = (ig[...].astype(jnp.float32) * val[...].astype(jnp.float32)).astype(jnp.bfloat16)
    tail[...] = product[rows_mix - 16 :, :]
    gated[8:, :] = product.astype(jnp.float32)

    expert_sub = lax.broadcasted_iota(jnp.int32, (PLANE, tokens), 0)
    t_sub = lax.broadcasted_iota(jnp.int32, (tokens, tokens), 0)
    t_lane = lax.broadcasted_iota(jnp.int32, (tokens, tokens), 1)
    earlier = jnp.where(t_sub < t_lane, 1.0, 0.0).astype(jnp.bfloat16)
    id0, id1 = ids_ref[0:1, :], ids_ref[1:2, :]
    hot0 = jnp.where(expert_sub == id0, 1.0, 0.0)
    hot1 = jnp.where(expert_sub == id1, 1.0, 0.0)
    before0 = jnp.dot(hot0.astype(jnp.bfloat16), earlier, preferred_element_type=jnp.float32)
    before1 = jnp.dot(hot1.astype(jnp.bfloat16), earlier, preferred_element_type=jnp.float32)
    before1 = before1 + jnp.sum(hot0, axis=1, keepdims=True)
    slot0 = jnp.sum(hot0 * before0, axis=0, keepdims=True)
    slot1 = jnp.sum(hot1 * before1, axis=0, keepdims=True)
    place0 = id0 * cap + slot0.astype(jnp.int32)
    place1 = id1 * cap + slot1.astype(jnp.int32)

    def fill(k):
        for block in range(PLANE * cap // 256):
            row = block * 256 + lax.broadcasted_iota(jnp.int32, (256, tokens), 0)
            hit = jnp.logical_or(row == place0, row == place1)
            outgoing[k, block * 256 : (block + 1) * 256, :] = jnp.dot(
                jnp.where(hit, 1.0, 0.0).astype(jnp.bfloat16),
                normed[:, k * COLS : (k + 1) * COLS],
                preferred_element_type=jnp.float32,
            ).astype(jnp.bfloat16)

    mine = pl.ds(pl.multiple_of(me * cap, cap), cap)

    def exchange(src, dst, k, send_sem, recv_sem):
        dst[k, mine, :] = src[k, mine, :]

        def one(step, _):
            j, pep, ptp = peer(step)
            send(
                src.at[k, pl.ds(pl.multiple_of(j * cap, cap), cap), :],
                dst.at[k, mine, :],
                send_sem.at[k],
                recv_sem.at[k],
                (pep, ptp),
            )
            return 0

        lax.fori_loop(1, PLANE, one, 0)

    def all_of(ref, k, sem):
        settle(ref.at[k, pl.ds(0, (PLANE - 1) * cap), :], sem.at[k])

    half = NZ // 2

    def pass_on(piece, t, sem):
        def one(number, other, way):
            slot = lax.rem(number, WINDOW)

            @pl.when(number >= WINDOW)
            def _():
                settle(piece, w_send.at[way, slot])

            send(piece, piece, w_send.at[way, slot], sem, (other, tp))

        for all_way, some_way, other, way in (
            (dist < half - 1, dist == half - 1, ahead, 0),
            (jnp.logical_or(dist == 0, dist > half + 1), dist == half + 1, behind, 1),
        ):

            @pl.when(all_way)
            def _():
                one(t, other, way)

            @pl.when(jnp.logical_and(some_way, lax.rem(t, 2) == way))
            def _():
                one(lax.div(t, 2), other, way)

    def serve(start, stop):
        def gate_up(t, _):
            settle(gu_at(t), w_sem.at[t])
            pass_on(gu_at(t), t, w_sem.at[t])
            return 0

        def downward(t, _):
            j, i = lax.div(t - gu_hops, d_hops), lax.rem(t - gu_hops, d_hops)
            settle(down_at(j, i), w_sem.at[t])
            pass_on(down_at(j, i), t, w_sem.at[t])
            return 0

        if start < gu_hops:
            lax.fori_loop(start, min(stop, gu_hops), gate_up, 0)
        if stop > gu_hops:
            lax.fori_loop(max(start, gu_hops), stop, downward, 0)

    def project(k, piece):
        def one(n, _):
            at = pl.ds(pl.multiple_of(n * 256, 256), 256)
            product = jnp.dot(rows[k, :, :], gu[k * COLS : (k + 1) * COLS, at], preferred_element_type=jnp.float32)
            if k == 0:
                acc[:, at] = product
            else:
                acc[:, at] += product
            return 0

        steps = 2 * inner // 256 // 2
        lax.fori_loop(piece * steps, (piece + 1) * steps, one, 0)

    def activate():
        def one(b, _):
            at = pl.ds(pl.multiple_of(b * 128, 128), 128)
            g, u = acc[at, 0:inner], acc[at, inner:]
            hidden[at, :] = (g * jax.nn.sigmoid(g) * u).astype(jnp.bfloat16)
            return 0

        lax.fori_loop(0, PLANE * cap // 128, one, 0)

    def produce(j):
        def one(n, _):
            at = pl.ds(pl.multiple_of(n * 256, 256), 256)
            results[j, :, at] = jnp.dot(hidden[...], down[j, :, at], preferred_element_type=jnp.float32).astype(
                jnp.bfloat16
            )
            return 0

        lax.fori_loop(0, COLS // 256, one, 0)

    def mix(j):
        all_of(returned, j, r_recv)
        total = jnp.dot(combine[0], returned[j], preferred_element_type=jnp.float32)
        total = total + jnp.dot(combine[1], returned[j], preferred_element_type=jnp.float32)
        out_ref[:, j * COLS : (j + 1) * COLS] = total.astype(jnp.bfloat16)
        columns = pl.ds(j * COLS, COLS)
        pltpu.make_async_copy(out_ref.at[:, columns], out_hbm.at[:, columns], out_sem.at[j]).start()

    def near(i):
        return lax.rem(y + 1 + i, NY) * NC + c

    def share_of(b, q):
        return project_w.at[b, pl.ds(pl.multiple_of(q * part, part), part), :]

    others = NY - 1
    three = project_w.at[0, pl.ds(0, others * part), :]
    three_wide = project_w.at[0, pl.ds(0, others * wide), :]

    def wide_of(b, q):
        return project_w.at[b, pl.ds(pl.multiple_of(split + q * wide, wide), wide), :]

    lone, whole = NZ + NX, NZ + NX + 1
    three_plain = project_w.at[0, pl.ds(0, others * plain), :]

    def plain_of(b):
        return project_w.at[b, pl.ds(width - plain, plain), :]

    def to_pair(q):
        def one(i, _):
            send(share_of(near(i), q), share_of(near(i), q), pair_send.at[q], pair_recv.at[q], (ep, pair))
            return 0

        lax.fori_loop(0, others, one, 0)

    def wide_to_pair(q):
        def one(i, _):
            send(wide_of(near(i), q), wide_of(near(i), q), pair_send.at[NZ + q], pair_recv.at[NZ + q], (ep, pair))
            return 0

        lax.fori_loop(0, others, one, 0)

    def along_x():
        settle(three_wide, share_sem.at[3])

        def one(t, _):
            far, i = lax.div(t, others), lax.rem(t, others)
            to = z * NX + lax.rem(x + 1 + far, NX)
            send(wide_of(near(i), x), wide_of(near(i), x), along_send.at[far], along_recv.at[far], (to, tp))
            return 0

        lax.fori_loop(0, (NX - 1) * others, one, 0)
        wide_to_pair(x)

    def from_x():
        for far in range(NX - 1):
            settle(three_wide, along_recv.at[far])
            wide_to_pair(lax.rem(x + NX - 1 - far, NX))

    def from_y():
        settle(three_plain, share_sem.at[5])

        def one(i, _):
            send(plain_of(near(i)), plain_of(near(i)), pair_send.at[lone], pair_recv.at[lone], (ep, pair))
            return 0

        lax.fori_loop(0, others, one, 0)

    def goes_up(i):
        return jnp.logical_or(i == 0, jnp.logical_and(i == 2, c == 0))

    def ring_send_piece(q, way, m, i):
        other = ahead if way == 0 else behind
        piece = share_of(near(i), q)
        send(piece, piece, ring_send.at[way, m, i], ring_recv.at[way, m, i], (other, tp))

    def ring_start():
        def one(i, _):
            for way in (0, 1):
                ring_send_piece(z, way, 0, i)
            return 0

        lax.fori_loop(0, others, one, 0)

    def ring_step(k):
        for way in (0, 1):
            q = lax.rem(z + NZ - k, NZ) if way == 0 else lax.rem(z + k, NZ)

            def one(i, _):
                settle(share_of(near(i), q), ring_recv.at[way, k - 1, i])
                if k < half - 1:
                    ring_send_piece(q, way, k, i)
                else:

                    @pl.when(goes_up(i) if way == 0 else jnp.logical_not(goes_up(i)))
                    def _():
                        ring_send_piece(q, way, k, i)

                return 0

            lax.fori_loop(0, others, one, 0)
            to_pair(q)

    def ring_last():
        q = lax.rem(z + half, NZ)

        def one(i, _):
            @pl.when(goes_up(i))
            def _():
                settle(share_of(near(i), q), ring_recv.at[0, half - 1, i])

            @pl.when(jnp.logical_not(goes_up(i)))
            def _():
                settle(share_of(near(i), q), ring_recv.at[1, half - 1, i])

            return 0

        lax.fori_loop(0, others, one, 0)
        to_pair(q)

    def mixer_wide():
        for q in range(NX):
            settle(three_wide, pair_recv.at[NZ + q])
        settle(three_plain, pair_recv.at[lone])

        def one(b, _):
            to = pl.ds(pl.multiple_of(b * block_cols, block_cols), block_cols)
            mixer_acc[:, to] = jnp.dot(
                mixed[:, split:], project_w[b, split:, :], preferred_element_type=jnp.float32
            )
            return 0

        lax.fori_loop(0, n_tp, one, 0)

    def mixer_part(q):
        settle(three, pair_recv.at[q])
        at = pl.ds(pl.multiple_of(q * part, part), part)

        def one(b, _):
            to = pl.ds(pl.multiple_of(b * block_cols, block_cols), block_cols)
            mixer_acc[:, to] += jnp.dot(mixed[:, at], project_w[b, at, :], preferred_element_type=jnp.float32)
            return 0

        lax.fori_loop(0, n_tp, one, 0)

    block_cols = project_w.shape[2]

    first = WINDOW
    for k in range(chunks):
        fill(k)

    margin = logits_ref[0:1, :] - logits_ref[1:2, :]
    weight0 = share_ref[...] * jax.nn.sigmoid(margin)
    weight1 = share_ref[...] * jax.nn.sigmoid(-margin)
    lane_rows = jnp.concatenate(
        [
            place0.astype(jnp.float32),
            place1.astype(jnp.float32),
            weight0,
            weight1,
            jnp.zeros((124, tokens), jnp.float32),
        ],
        axis=0,
    )
    turned = lane_rows.T
    cplace0, cplace1 = turned[:, 0:1].astype(jnp.int32), turned[:, 1:2].astype(jnp.int32)
    cweight0, cweight1 = turned[:, 2:3], turned[:, 3:4]
    for block in range(PLANE * cap // 256):
        column = block * 256 + lax.broadcasted_iota(jnp.int32, (tokens, 256), 1)
        weight = jnp.where(column == cplace0, cweight0, 0.0) + jnp.where(column == cplace1, cweight1, 0.0)
        coarse = weight.astype(jnp.bfloat16)
        combine[0, :, block * 256 : (block + 1) * 256] = coarse
        combine[1, :, block * 256 : (block + 1) * 256] = (weight - coarse.astype(jnp.float32)).astype(jnp.bfloat16)

    pl.semaphore_wait(barrier, PLANE - 1 + 4)
    send(tail, halo, halo_sem.at[0], halo_sem.at[1], (lax.div(later, n_tp), lax.rem(later, n_tp)))

    @pl.when(is_home)
    def _():
        serve(0, first)

    for k in range(chunks):
        exchange(outgoing, rows, k, x_send, x_recv)

    loads[3].wait()

    def give(i, _):
        for piece, k in ((share_of(tp, z), 0), (wide_of(tp, x), 2)):
            send(piece, piece, share_sem.at[k], share_sem.at[k + 1], (ep, near(i)))
        return 0

    lax.fori_loop(0, others, give, 0)

    def give_plain(i, _):
        send(plain_of(tp), plain_of(tp), share_sem.at[4], share_sem.at[5], (ep, near(i)))
        return 0

    lax.fori_loop(0, others, give_plain, 0)
    send(project_w.at[tp], project_w.at[tp], pair_send.at[whole], pair_recv.at[whole], (ep, pair))

    @pl.when(jnp.logical_not(is_home))
    def _():
        serve(0, first)

    def upto(fraction):
        return gu_hops * fraction // 32

    serve(first, upto(10))
    all_of(rows, 0, x_recv)
    project(0, 0)
    serve(upto(10), upto(11))
    project(0, 1)
    serve(upto(11), upto(13))

    settle(halo, halo_sem.at[1])
    loads[2].wait()
    seq_len = n_ep * n_tp * rows_mix // SEQS
    inside = lax.rem(flat * rows_mix, seq_len) != 0
    early = halo[...].astype(jnp.float32)[8:, :]
    gated[0:8, :] = jnp.where(inside, early, 0.0)

    def filter_columns(n, _):
        at = pl.ds(pl.multiple_of(n * 256, 256), 256)
        filtered = taps_ref[0:1, at] * gated[6 : 6 + rows_mix, at]
        filtered = filtered + taps_ref[1:2, at] * gated[7 : 7 + rows_mix, at]
        filtered = filtered + taps_ref[2:3, at] * gated[8 : 8 + rows_mix, at]
        mixed[:, at] = (og[:, at].astype(jnp.float32) * filtered).astype(jnp.bfloat16)
        return 0

    lax.fori_loop(0, width // 256, filter_columns, 0)

    serve(upto(13), upto(19))
    all_of(rows, 1, x_recv)
    project(1, 0)
    serve(upto(19), upto(20))
    project(1, 1)
    serve(upto(20), upto(27))
    all_of(rows, 2, x_recv)
    project(2, 0)
    serve(upto(27), upto(28))
    project(2, 1)
    serve(upto(28), gu_hops + d_hops // 2)
    all_of(rows, 3, x_recv)
    along_x()
    project(3, 0)
    serve(gu_hops + d_hops // 2, gu_hops + d_hops * 3 // 4)
    project(3, 1)
    serve(gu_hops + d_hops * 3 // 4, gu_hops + d_hops)
    activate()
    for j in range(chunks):
        if j > 0:
            serve(gu_hops + j * d_hops, gu_hops + (j + 1) * d_hops)
        if j == chunks - 1:
            settle(three, share_sem.at[1])
            ring_start()
        produce(j)
        exchange(results, returned, j, r_send, r_recv)

    to_pair(z)
    from_y()
    from_x()
    settle(project_w.at[tp], pair_recv.at[whole])
    ring_step(1)
    mix(0)
    mixer_wide()
    mixer_part(z)
    ring_step(2)
    mixer_part(lax.rem(z + NZ - 1, NZ))
    mixer_part(lax.rem(z + 1, NZ))
    ring_step(3)
    mix(1)
    mixer_part(lax.rem(z + NZ - 2, NZ))
    mixer_part(lax.rem(z + 2, NZ))
    ring_last()
    mixer_part(lax.rem(z + NZ - 3, NZ))
    mixer_part(lax.rem(z + 3, NZ))
    mix(2)
    mixer_part(lax.rem(z + half, NZ))
    mixer_ref[...] = mixer_acc[...].astype(jnp.bfloat16)
    mixer_out = pltpu.make_async_copy(mixer_ref, mixer_hbm, out_sem.at[chunks])
    mixer_out.start()
    mix(3)

    for k in range(chunks):
        all_of(outgoing, k, x_send)
        all_of(results, k, r_send)
    settle(tail, halo_sem.at[0])
    settle(three, share_sem.at[0])
    settle(three_wide, share_sem.at[2])
    settle(three_plain, share_sem.at[4])
    settle(three_plain, pair_send.at[lone])
    settle(project_w.at[tp], pair_send.at[whole])
    for q in range(NX):
        settle(three_wide, pair_send.at[NZ + q])
    for far in range(NX - 1):
        settle(three_wide, along_send.at[far])

    def pairs_left(q, _):
        settle(three, pair_send.at[q])
        return 0

    lax.fori_loop(0, NZ, pairs_left, 0)

    def rings_left(i, _):
        for way in (0, 1):
            for m in range(half - 1):
                settle(share_of(0, 0), ring_send.at[way, m, i])

        @pl.when(goes_up(i))
        def _():
            settle(share_of(0, 0), ring_send.at[0, half - 1, i])

        @pl.when(jnp.logical_not(goes_up(i)))
        def _():
            settle(share_of(0, 0), ring_send.at[1, half - 1, i])

        return 0

    lax.fori_loop(0, others, rings_left, 0)

    for sends, way in (
        (dist < half, 0),
        (jnp.logical_or(dist == 0, dist > half), 1),
    ):

        @pl.when(sends)
        def _():
            for slot in range(WINDOW):
                settle(gu_at(0), w_send.at[way, slot])

    mixer_out.wait()
    for j in range(chunks):
        columns = pl.ds(j * COLS, COLS)
        pltpu.make_async_copy(out_ref.at[:, columns], out_hbm.at[:, columns], out_sem.at[j]).wait()


def local(
    out_gate,
    in_gate,
    values,
    conv_taps,
    out_weight,
    expert_input,
    norm_gain,
    expert_ids,
    route_logits,
    group_share,
    gate_weight,
    up_weight,
    down_weight,
):
    tokens, width = expert_input.shape
    inner = gate_weight.shape[2]
    rows_mix = out_gate.shape[0]
    cap = 2 * tokens * expert_ids.shape[1] // PLANE
    chunks = width // COLS
    slots = PLANE * cap
    hops = width // GU_ROWS + chunks * (inner // D_ROWS)
    vmem = pl.BlockSpec(memory_space=pltpu.VMEM)
    hbm = pl.BlockSpec(memory_space=pl.ANY)
    bf, dma = jnp.bfloat16, pltpu.SemaphoreType.DMA
    return pl.pallas_call(
        step_kernel,
        out_shape=(
            jax.ShapeDtypeStruct((rows_mix, width), bf),
            jax.ShapeDtypeStruct((tokens, width), bf),
        ),
        in_specs=[vmem] * 6 + [hbm] * 7,
        out_specs=(hbm, hbm),
        scratch_shapes=[
            pltpu.VMEM((rows_mix, width), bf),
            pltpu.VMEM((tokens, width), bf),
            pltpu.VMEM((tokens, width), bf),
            pltpu.VMEM((2, tokens, slots), bf),
            pltpu.VMEM((chunks, slots, COLS), bf),
            pltpu.VMEM((chunks, slots, COLS), bf),
            pltpu.VMEM((width, 2 * inner), bf),
            pltpu.VMEM((chunks, inner, COLS), bf),
            pltpu.VMEM((slots, 2 * inner), jnp.float32),
            pltpu.VMEM((slots, inner), bf),
            pltpu.VMEM((chunks, slots, COLS), bf),
            pltpu.VMEM((chunks, slots, COLS), bf),
            pltpu.VMEM((rows_mix, width), bf),
            pltpu.VMEM((rows_mix, width), bf),
            pltpu.VMEM((rows_mix, width), bf),
            pltpu.VMEM((8 + rows_mix, width), jnp.float32),
            pltpu.VMEM((16, width), bf),
            pltpu.VMEM((16, width), bf),
            pltpu.VMEM((rows_mix, width), bf),
            pltpu.VMEM((NY * NC, *out_weight.shape), bf),
            pltpu.VMEM((rows_mix, width), jnp.float32),
            dma((hops,)),
            dma((2, WINDOW)),
            dma((chunks,)),
            dma((chunks,)),
            dma((chunks,)),
            dma((chunks,)),
            dma((4,)),
            dma((2,)),
            dma((6,)),
            dma((2, NZ // 2, NY - 1)),
            dma((2, NZ // 2, NY - 1)),
            dma((NZ + NX + 2,)),
            dma((NZ + NX + 2,)),
            dma((NX - 1,)),
            dma((NX - 1,)),
            dma((chunks + 1,)),
        ],
        compiler_params=pltpu.CompilerParams(
            collective_id=0, has_side_effects=True, vmem_limit_bytes=63 * 1024 * 1024
        ),
        name="layer_step",
    )(
        expert_input,
        norm_gain[None, :],
        expert_ids.T,
        route_logits.T,
        group_share[None, :],
        conv_taps,
        out_gate,
        in_gate,
        values,
        out_weight,
        gate_weight,
        up_weight,
        down_weight,
    )


def solution(mesh):
    return jax.shard_map(
        local,
        mesh=mesh,
        in_specs=(
            P(("ep", "tp"), None),
            P(("ep", "tp"), None),
            P(("ep", "tp"), None),
            P(),
            P(None, "tp"),
            P(("ep", "tp"), None),
            P(),
            P(("ep", "tp"), None),
            P(("ep", "tp"), None),
            P(("ep", "tp")),
            P("ep", None, None),
            P("ep", None, None),
            P("ep", None, None),
        ),
        out_specs=(P(("ep", "tp"), None), P(("ep", "tp"), None)),
        check_vma=False,
    )
```

```python
import functools

import jax
import jax.numpy as jnp
from jax import lax
from jax.experimental import pallas as pl
from jax.experimental.pallas import tpu as pltpu
from jax.sharding import PartitionSpec as P

SEQS = 1
norm_eps = 1e-05
MESH = pl.DeviceIdType.MESH

NX, NY, NZ, NC = 4, 4, 8, 2
PLANE = NX * NY * NC
COLS = 512
GU_ROWS = 32
D_ROWS = 64
WINDOW = 6


def step_kernel(
    x_ref,
    gain_ref,
    ids_ref,
    logits_ref,
    share_ref,
    taps_ref,
    og_hbm,
    ig_hbm,
    val_hbm,
    block_hbm,
    gate_hbm,
    up_hbm,
    down_hbm,
    mixer_ref,
    out_ref,
    normed,
    combine,
    outgoing,
    rows,
    gu,
    down,
    acc,
    hidden,
    results,
    returned,
    og,
    ig,
    val,
    gated,
    tail,
    halo,
    mixed,
    project_w,
    mixer_acc,
    w_sem,
    w_send,
    x_recv,
    x_send,
    r_recv,
    r_send,
    in_sem,
    halo_sem,
    share_sem,
    ring_recv,
    ring_send,
    pair_recv,
    pair_send,
    along_recv,
    along_send,
):
    tokens, width = x_ref.shape
    cap = outgoing.shape[1] // PLANE
    chunks = width // COLS
    inner = hidden.shape[1]
    gu_hops = width // GU_ROWS
    d_hops = inner // D_ROWS
    rows_mix = og.shape[0]
    split, plain = width // 2, width // 4
    part, wide = split // NZ, (width - split - plain) // NX

    ep, tp = lax.axis_index("ep"), lax.axis_index("tp")
    z, x = lax.div(ep, NX), lax.rem(ep, NX)
    y, c = lax.div(tp, NC), lax.rem(tp, NC)
    me = (c * NY + y) * NX + x
    ahead = lax.rem(z + 1, NZ) * NX + x
    behind = lax.rem(z + NZ - 1, NZ) * NX + x
    dist = lax.rem(z + NZ - (y + NY * c), NZ)
    is_home = dist == 0
    pair = y * NC + 1 - c
    n_ep, n_tp = NZ * NX, NY * NC
    flat = ep * n_tp + tp
    later = lax.rem(flat + 1, n_ep * n_tp)
    sooner = lax.rem(flat + n_ep * n_tp - 1, n_ep * n_tp)

    def peer(step):
        px = lax.rem(x + lax.rem(step, NX), NX)
        py = lax.rem(y + lax.rem(lax.div(step, NX), NY), NY)
        pc = lax.rem(c + lax.div(step, NX * NY), NC)
        return (pc * NY + py) * NX + px, z * NX + px, py * NC + pc

    def send(src, dst, send_sem, recv_sem, to):
        pltpu.make_async_remote_copy(
            src_ref=src,
            dst_ref=dst,
            send_sem=send_sem,
            recv_sem=recv_sem,
            device_id=to,
            device_id_type=MESH,
        ).start()

    def settle(ref, sem):
        pltpu.make_async_copy(ref, ref, sem).wait()

    def gu_at(i):
        return gu.at[pl.ds(pl.multiple_of(i * GU_ROWS, GU_ROWS), GU_ROWS), :]

    def down_at(j, i):
        return down.at[j, pl.ds(pl.multiple_of(i * D_ROWS, D_ROWS), D_ROWS), :]

    barrier = pltpu.get_barrier_semaphore()

    def greet(step, _):
        _, pep, ptp = peer(step)
        pl.semaphore_signal(barrier, inc=1, device_id=(pep, ptp), device_id_type=MESH)
        return 0

    lax.fori_loop(1, PLANE, greet, 0)
    for other in (ahead, behind):
        pl.semaphore_signal(barrier, inc=1, device_id=(other, tp), device_id_type=MESH)
    for other in (later, sooner):
        pl.semaphore_signal(
            barrier, inc=1, device_id=(lax.div(other, n_tp), lax.rem(other, n_tp)), device_id_type=MESH
        )

    @pl.when(is_home)
    def _():
        def load_gu(i, _):
            at = pl.ds(pl.multiple_of(i * GU_ROWS, GU_ROWS), GU_ROWS)
            pltpu.make_async_copy(gate_hbm.at[0, at, :], gu.at[at, pl.ds(0, inner)], w_sem.at[i]).start()
            pltpu.make_async_copy(up_hbm.at[0, at, :], gu.at[at, pl.ds(inner, inner)], w_sem.at[i]).start()
            return 0

        lax.fori_loop(0, gu_hops, load_gu, 0)
        for j in range(chunks):
            for i in range(d_hops):
                pltpu.make_async_copy(
                    down_hbm.at[0, pl.ds(i * D_ROWS, D_ROWS), pl.ds(j * COLS, COLS)],
                    down.at[j, pl.ds(i * D_ROWS, D_ROWS), :],
                    w_sem.at[gu_hops + j * d_hops + i],
                ).start()

    loads = [
        pltpu.make_async_copy(ig_hbm, ig, in_sem.at[0]),
        pltpu.make_async_copy(val_hbm, val, in_sem.at[1]),
        pltpu.make_async_copy(og_hbm, og, in_sem.at[2]),
        pltpu.make_async_copy(block_hbm, project_w.at[tp], in_sem.at[3]),
    ]
    for load in loads:
        load.start()

    xf = x_ref[...].astype(jnp.float32)
    scale = lax.rsqrt(jnp.mean(xf * xf, axis=-1, keepdims=True) + norm_eps)
    normed[...] = (xf * scale * gain_ref[...]).astype(jnp.bfloat16)

    loads[0].wait()
    loads[1].wait()
    product = (ig[...].astype(jnp.float32) * val[...].astype(jnp.float32)).astype(jnp.bfloat16)
    tail[...] = product[rows_mix - 16 :, :]
    gated[8:, :] = product.astype(jnp.float32)

    expert_sub = lax.broadcasted_iota(jnp.int32, (PLANE, tokens), 0)
    t_sub = lax.broadcasted_iota(jnp.int32, (tokens, tokens), 0)
    t_lane = lax.broadcasted_iota(jnp.int32, (tokens, tokens), 1)
    earlier = jnp.where(t_sub < t_lane, 1.0, 0.0).astype(jnp.bfloat16)
    id0, id1 = ids_ref[0:1, :], ids_ref[1:2, :]
    hot0 = jnp.where(expert_sub == id0, 1.0, 0.0)
    hot1 = jnp.where(expert_sub == id1, 1.0, 0.0)
    before0 = jnp.dot(hot0.astype(jnp.bfloat16), earlier, preferred_element_type=jnp.float32)
    before1 = jnp.dot(hot1.astype(jnp.bfloat16), earlier, preferred_element_type=jnp.float32)
    before1 = before1 + jnp.sum(hot0, axis=1, keepdims=True)
    slot0 = jnp.sum(hot0 * before0, axis=0, keepdims=True)
    slot1 = jnp.sum(hot1 * before1, axis=0, keepdims=True)
    place0 = id0 * cap + slot0.astype(jnp.int32)
    place1 = id1 * cap + slot1.astype(jnp.int32)

    def fill(k):
        for block in range(PLANE * cap // 256):
            row = block * 256 + lax.broadcasted_iota(jnp.int32, (256, tokens), 0)
            hit = jnp.logical_or(row == place0, row == place1)
            outgoing[k, block * 256 : (block + 1) * 256, :] = jnp.dot(
                jnp.where(hit, 1.0, 0.0).astype(jnp.bfloat16),
                normed[:, k * COLS : (k + 1) * COLS],
                preferred_element_type=jnp.float32,
            ).astype(jnp.bfloat16)

    mine = pl.ds(pl.multiple_of(me * cap, cap), cap)

    def exchange(src, dst, k, send_sem, recv_sem):
        dst[k, mine, :] = src[k, mine, :]

        def one(step, _):
            j, pep, ptp = peer(step)
            send(
                src.at[k, pl.ds(pl.multiple_of(j * cap, cap), cap), :],
                dst.at[k, mine, :],
                send_sem.at[k],
                recv_sem.at[k],
                (pep, ptp),
            )
            return 0

        lax.fori_loop(1, PLANE, one, 0)

    def all_of(ref, k, sem):
        settle(ref.at[k, pl.ds(0, (PLANE - 1) * cap), :], sem.at[k])

    half = NZ // 2

    def pass_on(piece, t, sem):
        def one(number, other, way):
            slot = lax.rem(number, WINDOW)

            @pl.when(number >= WINDOW)
            def _():
                settle(piece, w_send.at[way, slot])

            send(piece, piece, w_send.at[way, slot], sem, (other, tp))

        for all_way, some_way, other, way in (
            (dist < half - 1, dist == half - 1, ahead, 0),
            (jnp.logical_or(dist == 0, dist > half + 1), dist == half + 1, behind, 1),
        ):

            @pl.when(all_way)
            def _():
                one(t, other, way)

            @pl.when(jnp.logical_and(some_way, lax.rem(t, 2) == way))
            def _():
                one(lax.div(t, 2), other, way)

    def serve(start, stop):
        def gate_up(t, _):
            settle(gu_at(t), w_sem.at[t])
            pass_on(gu_at(t), t, w_sem.at[t])
            return 0

        def downward(t, _):
            j, i = lax.div(t - gu_hops, d_hops), lax.rem(t - gu_hops, d_hops)
            settle(down_at(j, i), w_sem.at[t])
            pass_on(down_at(j, i), t, w_sem.at[t])
            return 0

        if start < gu_hops:
            lax.fori_loop(start, min(stop, gu_hops), gate_up, 0)
        if stop > gu_hops:
            lax.fori_loop(max(start, gu_hops), stop, downward, 0)

    def project(k, piece):
        def one(n, _):
            at = pl.ds(pl.multiple_of(n * 256, 256), 256)
            product = jnp.dot(rows[k, :, :], gu[k * COLS : (k + 1) * COLS, at], preferred_element_type=jnp.float32)
            if k == 0:
                acc[:, at] = product
            else:
                acc[:, at] += product
            return 0

        steps = 2 * inner // 256 // 2
        lax.fori_loop(piece * steps, (piece + 1) * steps, one, 0)

    def activate():
        def one(b, _):
            at = pl.ds(pl.multiple_of(b * 128, 128), 128)
            g, u = acc[at, 0:inner], acc[at, inner:]
            hidden[at, :] = (g * jax.nn.sigmoid(g) * u).astype(jnp.bfloat16)
            return 0

        lax.fori_loop(0, PLANE * cap // 128, one, 0)

    def produce(j):
        def one(n, _):
            at = pl.ds(pl.multiple_of(n * 256, 256), 256)
            results[j, :, at] = jnp.dot(hidden[...], down[j, :, at], preferred_element_type=jnp.float32).astype(
                jnp.bfloat16
            )
            return 0

        lax.fori_loop(0, COLS // 256, one, 0)

    def mix(j):
        all_of(returned, j, r_recv)
        total = jnp.dot(combine[0], returned[j], preferred_element_type=jnp.float32)
        total = total + jnp.dot(combine[1], returned[j], preferred_element_type=jnp.float32)
        out_ref[:, j * COLS : (j + 1) * COLS] = total.astype(jnp.bfloat16)

    def near(i):
        return lax.rem(y + 1 + i, NY) * NC + c

    def share_of(b, q):
        return project_w.at[b, pl.ds(pl.multiple_of(q * part, part), part), :]

    others = NY - 1
    three = project_w.at[0, pl.ds(0, others * part), :]
    three_wide = project_w.at[0, pl.ds(0, others * wide), :]

    def wide_of(b, q):
        return project_w.at[b, pl.ds(pl.multiple_of(split + q * wide, wide), wide), :]

    lone, whole = NZ + NX, NZ + NX + 1
    three_plain = project_w.at[0, pl.ds(0, others * plain), :]

    def plain_of(b):
        return project_w.at[b, pl.ds(width - plain, plain), :]

    def to_pair(q):
        def one(i, _):
            send(share_of(near(i), q), share_of(near(i), q), pair_send.at[q], pair_recv.at[q], (ep, pair))
            return 0

        lax.fori_loop(0, others, one, 0)

    def wide_to_pair(q):
        def one(i, _):
            send(wide_of(near(i), q), wide_of(near(i), q), pair_send.at[NZ + q], pair_recv.at[NZ + q], (ep, pair))
            return 0

        lax.fori_loop(0, others, one, 0)

    def along_x():
        settle(three_wide, share_sem.at[3])

        def one(t, _):
            far, i = lax.div(t, others), lax.rem(t, others)
            to = z * NX + lax.rem(x + 1 + far, NX)
            send(wide_of(near(i), x), wide_of(near(i), x), along_send.at[far], along_recv.at[far], (to, tp))
            return 0

        lax.fori_loop(0, (NX - 1) * others, one, 0)
        wide_to_pair(x)

    def from_x():
        for far in range(NX - 1):
            settle(three_wide, along_recv.at[far])
            wide_to_pair(lax.rem(x + NX - 1 - far, NX))

    def from_y():
        settle(three_plain, share_sem.at[5])

        def one(i, _):
            send(plain_of(near(i)), plain_of(near(i)), pair_send.at[lone], pair_recv.at[lone], (ep, pair))
            return 0

        lax.fori_loop(0, others, one, 0)

    def goes_up(i):
        return jnp.logical_or(i == 0, jnp.logical_and(i == 2, c == 0))

    def ring_send_piece(q, way, m, i):
        other = ahead if way == 0 else behind
        piece = share_of(near(i), q)
        send(piece, piece, ring_send.at[way, m, i], ring_recv.at[way, m, i], (other, tp))

    def ring_start():
        def one(i, _):
            for way in (0, 1):
                ring_send_piece(z, way, 0, i)
            return 0

        lax.fori_loop(0, others, one, 0)

    def ring_step(k):
        for way in (0, 1):
            q = lax.rem(z + NZ - k, NZ) if way == 0 else lax.rem(z + k, NZ)

            def one(i, _):
                settle(share_of(near(i), q), ring_recv.at[way, k - 1, i])
                if k < half - 1:
                    ring_send_piece(q, way, k, i)
                else:

                    @pl.when(goes_up(i) if way == 0 else jnp.logical_not(goes_up(i)))
                    def _():
                        ring_send_piece(q, way, k, i)

                return 0

            lax.fori_loop(0, others, one, 0)
            to_pair(q)

    def ring_last():
        q = lax.rem(z + half, NZ)

        def one(i, _):
            @pl.when(goes_up(i))
            def _():
                settle(share_of(near(i), q), ring_recv.at[0, half - 1, i])

            @pl.when(jnp.logical_not(goes_up(i)))
            def _():
                settle(share_of(near(i), q), ring_recv.at[1, half - 1, i])

            return 0

        lax.fori_loop(0, others, one, 0)
        to_pair(q)

    def mixer_part(begin, end, last):
        def one(b, _):
            to = pl.ds(pl.multiple_of(b * block_cols, block_cols), block_cols)
            product = jnp.dot(mixed[:, begin:end], project_w[b, begin:end, :], preferred_element_type=jnp.float32)
            if last:
                mixer_ref[:, to] = (mixer_acc[:, to] + product).astype(jnp.bfloat16)
            else:
                mixer_acc[:, to] = product
            return 0

        lax.fori_loop(0, n_tp, one, 0)

    def mixer_second():
        for q in range(NX):
            settle(three_wide, pair_recv.at[NZ + q])
        settle(three_plain, pair_recv.at[lone])
        settle(project_w.at[tp], pair_recv.at[whole])
        mixer_part(split, width, False)

    def mixer_first():
        for q in range(NZ):
            settle(three, pair_recv.at[q])
        mixer_part(0, split, True)

    block_cols = project_w.shape[2]

    first = WINDOW
    for k in range(chunks):
        fill(k)

    margin = logits_ref[0:1, :] - logits_ref[1:2, :]
    weight0 = share_ref[...] * jax.nn.sigmoid(margin)
    weight1 = share_ref[...] * jax.nn.sigmoid(-margin)
    lane_rows = jnp.concatenate(
        [
            place0.astype(jnp.float32),
            place1.astype(jnp.float32),
            weight0,
            weight1,
            jnp.zeros((124, tokens), jnp.float32),
        ],
        axis=0,
    )
    turned = lane_rows.T
    cplace0, cplace1 = turned[:, 0:1].astype(jnp.int32), turned[:, 1:2].astype(jnp.int32)
    cweight0, cweight1 = turned[:, 2:3], turned[:, 3:4]
    for block in range(PLANE * cap // 256):
        column = block * 256 + lax.broadcasted_iota(jnp.int32, (tokens, 256), 1)
        weight = jnp.where(column == cplace0, cweight0, 0.0) + jnp.where(column == cplace1, cweight1, 0.0)
        coarse = weight.astype(jnp.bfloat16)
        combine[0, :, block * 256 : (block + 1) * 256] = coarse
        combine[1, :, block * 256 : (block + 1) * 256] = (weight - coarse.astype(jnp.float32)).astype(jnp.bfloat16)

    pl.semaphore_wait(barrier, PLANE - 1 + 4)
    send(tail, halo, halo_sem.at[0], halo_sem.at[1], (lax.div(later, n_tp), lax.rem(later, n_tp)))

    @pl.when(is_home)
    def _():
        serve(0, first)

    def give_wide(i, _):
        send(wide_of(tp, x), wide_of(tp, x), share_sem.at[2], share_sem.at[3], (ep, near(i)))
        return 0

    for k in range(chunks):
        exchange(outgoing, rows, k, x_send, x_recv)
        if k == 0:
            loads[3].wait()
            lax.fori_loop(0, others, give_wide, 0)

    def give(i, _):
        send(share_of(tp, z), share_of(tp, z), share_sem.at[0], share_sem.at[1], (ep, near(i)))
        return 0

    lax.fori_loop(0, others, give, 0)

    def give_plain(i, _):
        send(plain_of(tp), plain_of(tp), share_sem.at[4], share_sem.at[5], (ep, near(i)))
        return 0

    lax.fori_loop(0, others, give_plain, 0)
    send(project_w.at[tp], project_w.at[tp], pair_send.at[whole], pair_recv.at[whole], (ep, pair))

    @pl.when(jnp.logical_not(is_home))
    def _():
        serve(0, first)

    def upto(fraction):
        return gu_hops * fraction // 32

    serve(first, upto(14))

    settle(halo, halo_sem.at[1])
    loads[2].wait()
    seq_len = n_ep * n_tp * rows_mix // SEQS
    inside = lax.rem(flat * rows_mix, seq_len) != 0
    early = halo[...].astype(jnp.float32)[8:, :]
    gated[0:8, :] = jnp.where(inside, early, 0.0)

    def filter_columns(n, _):
        at = pl.ds(pl.multiple_of(n * 256, 256), 256)
        filtered = taps_ref[0:1, at] * gated[6 : 6 + rows_mix, at]
        filtered = filtered + taps_ref[1:2, at] * gated[7 : 7 + rows_mix, at]
        filtered = filtered + taps_ref[2:3, at] * gated[8 : 8 + rows_mix, at]
        mixed[:, at] = (og[:, at].astype(jnp.float32) * filtered).astype(jnp.bfloat16)
        return 0

    lax.fori_loop(0, width // 256, filter_columns, 0)

    serve(upto(14), upto(18))
    all_of(rows, 0, x_recv)
    project(0, 0)
    serve(upto(18), upto(19))
    project(0, 1)
    serve(upto(19), upto(26))
    along_x()
    serve(upto(26), upto(30))
    all_of(rows, 1, x_recv)
    project(1, 0)
    serve(upto(30), upto(31))
    project(1, 1)
    serve(upto(31), gu_hops + d_hops // 4)
    all_of(rows, 2, x_recv)
    project(2, 0)
    serve(gu_hops + d_hops // 4, gu_hops + d_hops // 2)
    project(2, 1)
    all_of(rows, 3, x_recv)
    project(3, 0)
    serve(gu_hops + d_hops // 2, gu_hops + d_hops * 3 // 4)
    project(3, 1)
    serve(gu_hops + d_hops * 3 // 4, gu_hops + d_hops)
    activate()
    for j in range(chunks):
        if j > 0:
            serve(gu_hops + j * d_hops, gu_hops + (j + 1) * d_hops)
        if j == chunks - 1:
            settle(three, share_sem.at[1])
            ring_start()
        produce(j)
        exchange(results, returned, j, r_send, r_recv)

    to_pair(z)
    ring_step(1)
    from_x()
    ring_step(2)
    ring_step(3)
    from_y()
    mix(0)
    ring_last()
    mixer_second()
    mix(1)
    mixer_first()
    mix(2)
    mix(3)

    for k in range(chunks):
        all_of(outgoing, k, x_send)
        all_of(results, k, r_send)
    settle(tail, halo_sem.at[0])
    settle(three, share_sem.at[0])
    settle(three_wide, share_sem.at[2])
    settle(three_plain, share_sem.at[4])
    settle(three_plain, pair_send.at[lone])
    settle(project_w.at[tp], pair_send.at[whole])
    for q in range(NX):
        settle(three_wide, pair_send.at[NZ + q])
    for far in range(NX - 1):
        settle(three_wide, along_send.at[far])

    def pairs_left(q, _):
        settle(three, pair_send.at[q])
        return 0

    lax.fori_loop(0, NZ, pairs_left, 0)

    def rings_left(i, _):
        for way in (0, 1):
            for m in range(half - 1):
                settle(share_of(0, 0), ring_send.at[way, m, i])

        @pl.when(goes_up(i))
        def _():
            settle(share_of(0, 0), ring_send.at[0, half - 1, i])

        @pl.when(jnp.logical_not(goes_up(i)))
        def _():
            settle(share_of(0, 0), ring_send.at[1, half - 1, i])

        return 0

    lax.fori_loop(0, others, rings_left, 0)

    for sends, way in (
        (dist < half, 0),
        (jnp.logical_or(dist == 0, dist > half), 1),
    ):

        @pl.when(sends)
        def _():
            for slot in range(WINDOW):
                settle(gu_at(0), w_send.at[way, slot])


def local(
    out_gate,
    in_gate,
    values,
    conv_taps,
    out_weight,
    expert_input,
    norm_gain,
    expert_ids,
    route_logits,
    group_share,
    gate_weight,
    up_weight,
    down_weight,
):
    tokens, width = expert_input.shape
    inner = gate_weight.shape[2]
    rows_mix = out_gate.shape[0]
    cap = 2 * tokens * expert_ids.shape[1] // PLANE
    chunks = width // COLS
    slots = PLANE * cap
    hops = width // GU_ROWS + chunks * (inner // D_ROWS)
    vmem = pl.BlockSpec(memory_space=pltpu.VMEM)
    hbm = pl.BlockSpec(memory_space=pltpu.HBM)
    bf, dma = jnp.bfloat16, pltpu.SemaphoreType.DMA
    return pl.pallas_call(
        step_kernel,
        out_shape=(
            jax.ShapeDtypeStruct((rows_mix, width), bf),
            jax.ShapeDtypeStruct((tokens, width), bf),
        ),
        in_specs=[vmem] * 6 + [hbm] * 7,
        out_specs=(vmem, vmem),
        scratch_shapes=[
            pltpu.VMEM((tokens, width), bf),
            pltpu.VMEM((2, tokens, slots), bf),
            pltpu.VMEM((chunks, slots, COLS), bf),
            pltpu.VMEM((chunks, slots, COLS), bf),
            pltpu.VMEM((width, 2 * inner), bf),
            pltpu.VMEM((chunks, inner, COLS), bf),
            pltpu.VMEM((slots, 2 * inner), jnp.float32),
            pltpu.VMEM((slots, inner), bf),
            pltpu.VMEM((chunks, slots, COLS), bf),
            pltpu.VMEM((chunks, slots, COLS), bf),
            pltpu.VMEM((rows_mix, width), bf),
            pltpu.VMEM((rows_mix, width), bf),
            pltpu.VMEM((rows_mix, width), bf),
            pltpu.VMEM((8 + rows_mix, width), jnp.float32),
            pltpu.VMEM((16, width), bf),
            pltpu.VMEM((16, width), bf),
            pltpu.VMEM((rows_mix, width), bf),
            pltpu.VMEM((NY * NC, *out_weight.shape), bf),
            pltpu.VMEM((rows_mix, width), jnp.float32),
            dma((hops,)),
            dma((2, WINDOW)),
            dma((chunks,)),
            dma((chunks,)),
            dma((chunks,)),
            dma((chunks,)),
            dma((4,)),
            dma((2,)),
            dma((6,)),
            dma((2, NZ // 2, NY - 1)),
            dma((2, NZ // 2, NY - 1)),
            dma((NZ + NX + 2,)),
            dma((NZ + NX + 2,)),
            dma((NX - 1,)),
            dma((NX - 1,)),
        ],
        compiler_params=pltpu.CompilerParams(
            collective_id=0, has_side_effects=True, vmem_limit_bytes=48 * 1024 * 1024
        ),
        name="layer_step",
    )(*(pltpu.with_memory_space_constraint(value, pltpu.HBM) for value in (
        expert_input,
        norm_gain[None, :],
        expert_ids.T,
        route_logits.T,
        group_share[None, :],
        conv_taps,
        out_gate,
        in_gate,
        values,
        out_weight,
        gate_weight,
        up_weight,
        down_weight,
    )))


def solution(mesh):
    return jax.shard_map(
        local,
        mesh=mesh,
        in_specs=(
            P(("ep", "tp"), None),
            P(("ep", "tp"), None),
            P(("ep", "tp"), None),
            P(),
            P(None, "tp"),
            P(("ep", "tp"), None),
            P(),
            P(("ep", "tp"), None),
            P(("ep", "tp"), None),
            P(("ep", "tp")),
            P("ep", None, None),
            P("ep", None, None),
            P("ep", None, None),
        ),
        out_specs=(P(("ep", "tp"), None), P(("ep", "tp"), None)),
        check_vma=False,
    )
```

```python
import functools

import jax
import jax.numpy as jnp
from jax import lax
from jax.experimental import pallas as pl
from jax.experimental.pallas import tpu as pltpu
from jax.sharding import PartitionSpec as P

SEQS = 1
norm_eps = 1e-05
MESH = pl.DeviceIdType.MESH

NX, NY, NZ, NC = 4, 4, 8, 2
PLANE = NX * NY * NC
COLS = 512
GU_ROWS = 32
D_ROWS = 64
WINDOW = 6


def step_kernel(
    x_ref,
    gain_ref,
    ids_ref,
    logits_ref,
    share_ref,
    taps_ref,
    og_hbm,
    ig_hbm,
    val_hbm,
    block_hbm,
    gate_hbm,
    up_hbm,
    down_hbm,
    mixer_ref,
    out_ref,
    normed,
    combine,
    outgoing,
    rows,
    gu,
    down,
    acc,
    hidden,
    results,
    returned,
    og,
    ig,
    val,
    gated,
    tail,
    halo,
    mixed,
    project_w,
    mixer_acc,
    w_sem,
    w_send,
    x_recv,
    x_send,
    r_recv,
    r_send,
    in_sem,
    halo_sem,
    share_sem,
    ring_recv,
    ring_send,
    pair_recv,
    pair_send,
    along_recv,
    along_send,
):
    tokens, width = x_ref.shape
    cap = outgoing.shape[1] // PLANE
    chunks = width // COLS
    inner = hidden.shape[1]
    gu_hops = width // GU_ROWS
    d_hops = inner // D_ROWS
    rows_mix = og.shape[0]
    split, plain = width // 2, width // 4
    part, wide = split // NZ, (width - split - plain) // NX

    ep, tp = lax.axis_index("ep"), lax.axis_index("tp")
    z, x = lax.div(ep, NX), lax.rem(ep, NX)
    y, c = lax.div(tp, NC), lax.rem(tp, NC)
    me = (c * NY + y) * NX + x
    ahead = lax.rem(z + 1, NZ) * NX + x
    behind = lax.rem(z + NZ - 1, NZ) * NX + x
    dist = lax.rem(z + NZ - (y + NY * c), NZ)
    is_home = dist == 0
    pair = y * NC + 1 - c
    n_ep, n_tp = NZ * NX, NY * NC
    flat = ep * n_tp + tp
    later = lax.rem(flat + 1, n_ep * n_tp)
    sooner = lax.rem(flat + n_ep * n_tp - 1, n_ep * n_tp)

    def peer(step):
        px = lax.rem(x + lax.rem(step, NX), NX)
        py = lax.rem(y + lax.rem(lax.div(step, NX), NY), NY)
        pc = lax.rem(c + lax.div(step, NX * NY), NC)
        return (pc * NY + py) * NX + px, z * NX + px, py * NC + pc

    def send(src, dst, send_sem, recv_sem, to):
        pltpu.make_async_remote_copy(
            src_ref=src,
            dst_ref=dst,
            send_sem=send_sem,
            recv_sem=recv_sem,
            device_id=to,
            device_id_type=MESH,
        ).start()

    def settle(ref, sem):
        pltpu.make_async_copy(ref, ref, sem).wait()

    def gu_at(i):
        return gu.at[pl.ds(pl.multiple_of(i * GU_ROWS, GU_ROWS), GU_ROWS), :]

    def down_at(j, i):
        return down.at[j, pl.ds(pl.multiple_of(i * D_ROWS, D_ROWS), D_ROWS), :]

    barrier = pltpu.get_barrier_semaphore()

    def greet(step, _):
        _, pep, ptp = peer(step)
        pl.semaphore_signal(barrier, inc=1, device_id=(pep, ptp), device_id_type=MESH)
        return 0

    lax.fori_loop(1, PLANE, greet, 0)
    for other in (ahead, behind):
        pl.semaphore_signal(barrier, inc=1, device_id=(other, tp), device_id_type=MESH)
    for other in (later, sooner):
        pl.semaphore_signal(
            barrier, inc=1, device_id=(lax.div(other, n_tp), lax.rem(other, n_tp)), device_id_type=MESH
        )

    @pl.when(is_home)
    def _():
        def load_gu(i, _):
            at = pl.ds(pl.multiple_of(i * GU_ROWS, GU_ROWS), GU_ROWS)
            pltpu.make_async_copy(gate_hbm.at[0, at, :], gu.at[at, pl.ds(0, inner)], w_sem.at[i]).start()
            pltpu.make_async_copy(up_hbm.at[0, at, :], gu.at[at, pl.ds(inner, inner)], w_sem.at[i]).start()
            return 0

        lax.fori_loop(0, gu_hops, load_gu, 0)
        for j in range(chunks):
            for i in range(d_hops):
                pltpu.make_async_copy(
                    down_hbm.at[0, pl.ds(i * D_ROWS, D_ROWS), pl.ds(j * COLS, COLS)],
                    down.at[j, pl.ds(i * D_ROWS, D_ROWS), :],
                    w_sem.at[gu_hops + j * d_hops + i],
                ).start()

    loads = [
        pltpu.make_async_copy(ig_hbm, ig, in_sem.at[0]),
        pltpu.make_async_copy(val_hbm, val, in_sem.at[1]),
        pltpu.make_async_copy(og_hbm, og, in_sem.at[2]),
        pltpu.make_async_copy(block_hbm, project_w.at[tp], in_sem.at[3]),
    ]
    for load in loads:
        load.start()

    xf = x_ref[...].astype(jnp.float32)
    scale = lax.rsqrt(jnp.mean(xf * xf, axis=-1, keepdims=True) + norm_eps)
    normed[...] = (xf * scale * gain_ref[...]).astype(jnp.bfloat16)

    loads[0].wait()
    loads[1].wait()
    product = (ig[...].astype(jnp.float32) * val[...].astype(jnp.float32)).astype(jnp.bfloat16)
    tail[...] = product[rows_mix - 16 :, :]
    gated[8:, :] = product.astype(jnp.float32)

    expert_sub = lax.broadcasted_iota(jnp.int32, (PLANE, tokens), 0)
    t_sub = lax.broadcasted_iota(jnp.int32, (tokens, tokens), 0)
    t_lane = lax.broadcasted_iota(jnp.int32, (tokens, tokens), 1)
    earlier = jnp.where(t_sub < t_lane, 1.0, 0.0).astype(jnp.bfloat16)
    id0, id1 = ids_ref[0:1, :], ids_ref[1:2, :]
    hot0 = jnp.where(expert_sub == id0, 1.0, 0.0)
    hot1 = jnp.where(expert_sub == id1, 1.0, 0.0)
    before0 = jnp.dot(hot0.astype(jnp.bfloat16), earlier, preferred_element_type=jnp.float32)
    before1 = jnp.dot(hot1.astype(jnp.bfloat16), earlier, preferred_element_type=jnp.float32)
    before1 = before1 + jnp.sum(hot0, axis=1, keepdims=True)
    slot0 = jnp.sum(hot0 * before0, axis=0, keepdims=True)
    slot1 = jnp.sum(hot1 * before1, axis=0, keepdims=True)
    place0 = id0 * cap + slot0.astype(jnp.int32)
    place1 = id1 * cap + slot1.astype(jnp.int32)

    def fill(k):
        for block in range(PLANE * cap // 256):
            row = block * 256 + lax.broadcasted_iota(jnp.int32, (256, tokens), 0)
            hit = jnp.logical_or(row == place0, row == place1)
            outgoing[k, block * 256 : (block + 1) * 256, :] = jnp.dot(
                jnp.where(hit, 1.0, 0.0).astype(jnp.bfloat16),
                normed[:, k * COLS : (k + 1) * COLS],
                preferred_element_type=jnp.float32,
            ).astype(jnp.bfloat16)

    mine = pl.ds(pl.multiple_of(me * cap, cap), cap)

    def exchange(src, dst, k, send_sem, recv_sem):
        dst[k, mine, :] = src[k, mine, :]

        def one(step, _):
            j, pep, ptp = peer(step)
            send(
                src.at[k, pl.ds(pl.multiple_of(j * cap, cap), cap), :],
                dst.at[k, mine, :],
                send_sem.at[k],
                recv_sem.at[k],
                (pep, ptp),
            )
            return 0

        lax.fori_loop(1, PLANE, one, 0)

    def all_of(ref, k, sem):
        settle(ref.at[k, pl.ds(0, (PLANE - 1) * cap), :], sem.at[k])

    half = NZ // 2

    def pass_on(piece, t, sem):
        def one(number, other, way):
            slot = lax.rem(number, WINDOW)

            @pl.when(number >= WINDOW)
            def _():
                settle(piece, w_send.at[way, slot])

            send(piece, piece, w_send.at[way, slot], sem, (other, tp))

        for all_way, some_way, other, way in (
            (dist < half - 1, dist == half - 1, ahead, 0),
            (jnp.logical_or(dist == 0, dist > half + 1), dist == half + 1, behind, 1),
        ):

            @pl.when(all_way)
            def _():
                one(t, other, way)

            @pl.when(jnp.logical_and(some_way, lax.rem(t, 2) == way))
            def _():
                one(lax.div(t, 2), other, way)

    def serve(start, stop):
        def gate_up(t, _):
            settle(gu_at(t), w_sem.at[t])
            pass_on(gu_at(t), t, w_sem.at[t])
            return 0

        def downward(t, _):
            j, i = lax.div(t - gu_hops, d_hops), lax.rem(t - gu_hops, d_hops)
            settle(down_at(j, i), w_sem.at[t])
            pass_on(down_at(j, i), t, w_sem.at[t])
            return 0

        if start < gu_hops:
            lax.fori_loop(start, min(stop, gu_hops), gate_up, 0)
        if stop > gu_hops:
            lax.fori_loop(max(start, gu_hops), stop, downward, 0)

    def project(k, piece):
        def one(n, _):
            at = pl.ds(pl.multiple_of(n * 256, 256), 256)
            product = jnp.dot(rows[k, :, :], gu[k * COLS : (k + 1) * COLS, at], preferred_element_type=jnp.float32)
            if k == 0:
                acc[:, at] = product
            else:
                acc[:, at] += product
            return 0

        steps = 2 * inner // 256 // 2
        lax.fori_loop(piece * steps, (piece + 1) * steps, one, 0)

    def activate():
        def one(b, _):
            at = pl.ds(pl.multiple_of(b * 128, 128), 128)
            g, u = acc[at, 0:inner], acc[at, inner:]
            hidden[at, :] = (g * jax.nn.sigmoid(g) * u).astype(jnp.bfloat16)
            return 0

        lax.fori_loop(0, PLANE * cap // 128, one, 0)

    def produce(j):
        def one(n, _):
            at = pl.ds(pl.multiple_of(n * 256, 256), 256)
            results[j, :, at] = jnp.dot(hidden[...], down[j, :, at], preferred_element_type=jnp.float32).astype(
                jnp.bfloat16
            )
            return 0

        lax.fori_loop(0, COLS // 256, one, 0)

    def mix(j):
        all_of(returned, j, r_recv)
        total = jnp.dot(combine[0], returned[j], preferred_element_type=jnp.float32)
        total = total + jnp.dot(combine[1], returned[j], preferred_element_type=jnp.float32)
        out_ref[:, j * COLS : (j + 1) * COLS] = total.astype(jnp.bfloat16)

    def near(i):
        return lax.rem(y + 1 + i, NY) * NC + c

    def share_of(b, q):
        return project_w.at[b, pl.ds(pl.multiple_of(q * part, part), part), :]

    others = NY - 1
    three = project_w.at[0, pl.ds(0, others * part), :]
    three_wide = project_w.at[0, pl.ds(0, others * wide), :]

    def wide_of(b, q):
        return project_w.at[b, pl.ds(pl.multiple_of(split + q * wide, wide), wide), :]

    lone, whole = NZ + NX, NZ + NX + 1
    three_plain = project_w.at[0, pl.ds(0, others * plain), :]

    def plain_of(b):
        return project_w.at[b, pl.ds(width - plain, plain), :]

    def to_pair(q):
        def one(i, _):
            send(share_of(near(i), q), share_of(near(i), q), pair_send.at[q], pair_recv.at[q], (ep, pair))
            return 0

        lax.fori_loop(0, others, one, 0)

    def wide_to_pair(q):
        def one(i, _):
            send(wide_of(near(i), q), wide_of(near(i), q), pair_send.at[NZ + q], pair_recv.at[NZ + q], (ep, pair))
            return 0

        lax.fori_loop(0, others, one, 0)

    def along_x():
        settle(three_wide, share_sem.at[3])

        def one(t, _):
            far, i = lax.div(t, others), lax.rem(t, others)
            to = z * NX + lax.rem(x + 1 + far, NX)
            send(wide_of(near(i), x), wide_of(near(i), x), along_send.at[far], along_recv.at[far], (to, tp))
            return 0

        lax.fori_loop(0, (NX - 1) * others, one, 0)
        wide_to_pair(x)

    def from_x():
        for far in range(NX - 1):
            settle(three_wide, along_recv.at[far])
            wide_to_pair(lax.rem(x + NX - 1 - far, NX))

    def from_y():
        settle(three_plain, share_sem.at[5])

        def one(i, _):
            send(plain_of(near(i)), plain_of(near(i)), pair_send.at[lone], pair_recv.at[lone], (ep, pair))
            return 0

        lax.fori_loop(0, others, one, 0)

    def goes_up(i):
        return jnp.logical_or(i == 0, jnp.logical_and(i == 2, c == 0))

    def ring_send_piece(q, way, m, i):
        other = ahead if way == 0 else behind
        piece = share_of(near(i), q)
        send(piece, piece, ring_send.at[way, m, i], ring_recv.at[way, m, i], (other, tp))

    def ring_start():
        def one(i, _):
            for way in (0, 1):
                ring_send_piece(z, way, 0, i)
            return 0

        lax.fori_loop(0, others, one, 0)

    def ring_step(k):
        for way in (0, 1):
            q = lax.rem(z + NZ - k, NZ) if way == 0 else lax.rem(z + k, NZ)

            def one(i, _):
                settle(share_of(near(i), q), ring_recv.at[way, k - 1, i])
                if k < half - 1:
                    ring_send_piece(q, way, k, i)
                else:

                    @pl.when(goes_up(i) if way == 0 else jnp.logical_not(goes_up(i)))
                    def _():
                        ring_send_piece(q, way, k, i)

                return 0

            lax.fori_loop(0, others, one, 0)
            to_pair(q)

    def ring_last():
        q = lax.rem(z + half, NZ)

        def one(i, _):
            @pl.when(goes_up(i))
            def _():
                settle(share_of(near(i), q), ring_recv.at[0, half - 1, i])

            @pl.when(jnp.logical_not(goes_up(i)))
            def _():
                settle(share_of(near(i), q), ring_recv.at[1, half - 1, i])

            return 0

        lax.fori_loop(0, others, one, 0)
        to_pair(q)

    def mixer_part(begin, end, last):
        def one(b, _):
            to = pl.ds(pl.multiple_of(b * block_cols, block_cols), block_cols)
            product = jnp.dot(mixed[:, begin:end], project_w[b, begin:end, :], preferred_element_type=jnp.float32)
            if last:
                mixer_ref[:, to] = (mixer_acc[:, to] + product).astype(jnp.bfloat16)
            else:
                mixer_acc[:, to] = product
            return 0

        lax.fori_loop(0, n_tp, one, 0)

    def mixer_second():
        for q in range(NX):
            settle(three_wide, pair_recv.at[NZ + q])
        settle(three_plain, pair_recv.at[lone])
        settle(project_w.at[tp], pair_recv.at[whole])
        mixer_part(split, width, False)

    def mixer_first():
        for q in range(NZ):
            settle(three, pair_recv.at[q])
        mixer_part(0, split, True)

    block_cols = project_w.shape[2]

    first = WINDOW
    for k in range(chunks):
        fill(k)

    margin = logits_ref[0:1, :] - logits_ref[1:2, :]
    weight0 = share_ref[...] * jax.nn.sigmoid(margin)
    weight1 = share_ref[...] * jax.nn.sigmoid(-margin)
    lane_rows = jnp.concatenate(
        [
            place0.astype(jnp.float32),
            place1.astype(jnp.float32),
            weight0,
            weight1,
            jnp.zeros((124, tokens), jnp.float32),
        ],
        axis=0,
    )
    turned = lane_rows.T
    cplace0, cplace1 = turned[:, 0:1].astype(jnp.int32), turned[:, 1:2].astype(jnp.int32)
    cweight0, cweight1 = turned[:, 2:3], turned[:, 3:4]
    for block in range(PLANE * cap // 256):
        column = block * 256 + lax.broadcasted_iota(jnp.int32, (tokens, 256), 1)
        weight = jnp.where(column == cplace0, cweight0, 0.0) + jnp.where(column == cplace1, cweight1, 0.0)
        coarse = weight.astype(jnp.bfloat16)
        combine[0, :, block * 256 : (block + 1) * 256] = coarse
        combine[1, :, block * 256 : (block + 1) * 256] = (weight - coarse.astype(jnp.float32)).astype(jnp.bfloat16)

    pl.semaphore_wait(barrier, PLANE - 1 + 4)
    send(tail, halo, halo_sem.at[0], halo_sem.at[1], (lax.div(later, n_tp), lax.rem(later, n_tp)))

    @pl.when(is_home)
    def _():
        serve(0, first)

    def give_wide(i, _):
        send(wide_of(tp, x), wide_of(tp, x), share_sem.at[2], share_sem.at[3], (ep, near(i)))
        return 0

    for k in range(chunks):
        exchange(outgoing, rows, k, x_send, x_recv)
        if k == 0:
            loads[3].wait()
            lax.fori_loop(0, others, give_wide, 0)

    def give(i, _):
        send(share_of(tp, z), share_of(tp, z), share_sem.at[0], share_sem.at[1], (ep, near(i)))
        return 0

    lax.fori_loop(0, others, give, 0)

    def give_plain(i, _):
        send(plain_of(tp), plain_of(tp), share_sem.at[4], share_sem.at[5], (ep, near(i)))
        return 0

    lax.fori_loop(0, others, give_plain, 0)
    send(project_w.at[tp], project_w.at[tp], pair_send.at[whole], pair_recv.at[whole], (ep, pair))

    @pl.when(jnp.logical_not(is_home))
    def _():
        serve(0, first)

    def upto(fraction):
        return gu_hops * fraction // 32

    serve(first, upto(14))

    settle(halo, halo_sem.at[1])
    loads[2].wait()
    seq_len = n_ep * n_tp * rows_mix // SEQS
    inside = lax.rem(flat * rows_mix, seq_len) != 0
    early = halo[...].astype(jnp.float32)[8:, :]
    gated[0:8, :] = jnp.where(inside, early, 0.0)

    def filter_columns(n, _):
        at = pl.ds(pl.multiple_of(n * 256, 256), 256)
        filtered = taps_ref[0:1, at] * gated[6 : 6 + rows_mix, at]
        filtered = filtered + taps_ref[1:2, at] * gated[7 : 7 + rows_mix, at]
        filtered = filtered + taps_ref[2:3, at] * gated[8 : 8 + rows_mix, at]
        mixed[:, at] = (og[:, at].astype(jnp.float32) * filtered).astype(jnp.bfloat16)
        return 0

    lax.fori_loop(0, width // 256, filter_columns, 0)

    serve(upto(14), upto(18))
    all_of(rows, 0, x_recv)
    project(0, 0)
    serve(upto(18), upto(19))
    project(0, 1)
    serve(upto(19), upto(26))
    along_x()
    serve(upto(26), upto(30))
    all_of(rows, 1, x_recv)
    project(1, 0)
    serve(upto(30), upto(31))
    project(1, 1)
    serve(upto(31), gu_hops + d_hops // 4)
    all_of(rows, 2, x_recv)
    project(2, 0)
    serve(gu_hops + d_hops // 4, gu_hops + d_hops // 2)
    project(2, 1)
    all_of(rows, 3, x_recv)
    project(3, 0)
    serve(gu_hops + d_hops // 2, gu_hops + d_hops * 3 // 4)
    project(3, 1)
    serve(gu_hops + d_hops * 3 // 4, gu_hops + d_hops)
    activate()
    for j in range(chunks):
        if j > 0:
            serve(gu_hops + j * d_hops, gu_hops + (j + 1) * d_hops)
        if j == chunks - 1:
            settle(three, share_sem.at[1])
            ring_start()
        produce(j)
        exchange(results, returned, j, r_send, r_recv)

    to_pair(z)
    ring_step(1)
    from_x()
    ring_step(2)
    ring_step(3)
    from_y()
    mix(0)
    ring_last()
    mixer_second()
    mix(1)
    mixer_first()
    mix(2)
    for k in range(chunks):
        all_of(outgoing, k, x_send)
        all_of(results, k, r_send)
    settle(tail, halo_sem.at[0])
    settle(three, share_sem.at[0])
    settle(three_wide, share_sem.at[2])
    settle(three_plain, share_sem.at[4])
    settle(three_plain, pair_send.at[lone])
    settle(project_w.at[tp], pair_send.at[whole])
    for q in range(NX):
        settle(three_wide, pair_send.at[NZ + q])
    for far in range(NX - 1):
        settle(three_wide, along_send.at[far])

    def pairs_left(q, _):
        settle(three, pair_send.at[q])
        return 0

    lax.fori_loop(0, NZ, pairs_left, 0)

    def rings_left(i, _):
        for way in (0, 1):
            for m in range(half - 1):
                settle(share_of(0, 0), ring_send.at[way, m, i])

        @pl.when(goes_up(i))
        def _():
            settle(share_of(0, 0), ring_send.at[0, half - 1, i])

        @pl.when(jnp.logical_not(goes_up(i)))
        def _():
            settle(share_of(0, 0), ring_send.at[1, half - 1, i])

        return 0

    lax.fori_loop(0, others, rings_left, 0)

    for sends, way in (
        (dist < half, 0),
        (jnp.logical_or(dist == 0, dist > half), 1),
    ):

        @pl.when(sends)
        def _():
            for slot in range(WINDOW):
                settle(gu_at(0), w_send.at[way, slot])

    mix(3)


def local(
    out_gate,
    in_gate,
    values,
    conv_taps,
    out_weight,
    expert_input,
    norm_gain,
    expert_ids,
    route_logits,
    group_share,
    gate_weight,
    up_weight,
    down_weight,
):
    tokens, width = expert_input.shape
    inner = gate_weight.shape[2]
    rows_mix = out_gate.shape[0]
    cap = 2 * tokens * expert_ids.shape[1] // PLANE
    chunks = width // COLS
    slots = PLANE * cap
    hops = width // GU_ROWS + chunks * (inner // D_ROWS)
    vmem = pl.BlockSpec(memory_space=pltpu.VMEM)
    hbm = pl.BlockSpec(memory_space=pltpu.HBM)
    bf, dma = jnp.bfloat16, pltpu.SemaphoreType.DMA
    return pl.pallas_call(
        step_kernel,
        out_shape=(
            jax.ShapeDtypeStruct((rows_mix, width), bf),
            jax.ShapeDtypeStruct((tokens, width), bf),
        ),
        in_specs=[vmem] * 6 + [hbm] * 7,
        out_specs=(vmem, vmem),
        scratch_shapes=[
            pltpu.VMEM((tokens, width), bf),
            pltpu.VMEM((2, tokens, slots), bf),
            pltpu.VMEM((chunks, slots, COLS), bf),
            pltpu.VMEM((chunks, slots, COLS), bf),
            pltpu.VMEM((width, 2 * inner), bf),
            pltpu.VMEM((chunks, inner, COLS), bf),
            pltpu.VMEM((slots, 2 * inner), jnp.float32),
            pltpu.VMEM((slots, inner), bf),
            pltpu.VMEM((chunks, slots, COLS), bf),
            pltpu.VMEM((chunks, slots, COLS), bf),
            pltpu.VMEM((rows_mix, width), bf),
            pltpu.VMEM((rows_mix, width), bf),
            pltpu.VMEM((rows_mix, width), bf),
            pltpu.VMEM((8 + rows_mix, width), jnp.float32),
            pltpu.VMEM((16, width), bf),
            pltpu.VMEM((16, width), bf),
            pltpu.VMEM((rows_mix, width), bf),
            pltpu.VMEM((NY * NC, *out_weight.shape), bf),
            pltpu.VMEM((rows_mix, width), jnp.float32),
            dma((hops,)),
            dma((2, WINDOW)),
            dma((chunks,)),
            dma((chunks,)),
            dma((chunks,)),
            dma((chunks,)),
            dma((4,)),
            dma((2,)),
            dma((6,)),
            dma((2, NZ // 2, NY - 1)),
            dma((2, NZ // 2, NY - 1)),
            dma((NZ + NX + 2,)),
            dma((NZ + NX + 2,)),
            dma((NX - 1,)),
            dma((NX - 1,)),
        ],
        compiler_params=pltpu.CompilerParams(
            collective_id=0, has_side_effects=True, vmem_limit_bytes=48 * 1024 * 1024
        ),
        name="layer_step",
    )(*(pltpu.with_memory_space_constraint(value, pltpu.HBM) for value in (
        expert_input,
        norm_gain[None, :],
        expert_ids.T,
        route_logits.T,
        group_share[None, :],
        conv_taps,
        out_gate,
        in_gate,
        values,
        out_weight,
        gate_weight,
        up_weight,
        down_weight,
    )))


def solution(mesh):
    return jax.shard_map(
        local,
        mesh=mesh,
        in_specs=(
            P(("ep", "tp"), None),
            P(("ep", "tp"), None),
            P(("ep", "tp"), None),
            P(),
            P(None, "tp"),
            P(("ep", "tp"), None),
            P(),
            P(("ep", "tp"), None),
            P(("ep", "tp"), None),
            P(("ep", "tp")),
            P("ep", None, None),
            P("ep", None, None),
            P("ep", None, None),
        ),
        out_specs=(P(("ep", "tp"), None), P(("ep", "tp"), None)),
        check_vma=False,
    )
```

```python
import functools

import jax
import jax.numpy as jnp
from jax import lax
from jax.experimental import pallas as pl
from jax.experimental.pallas import tpu as pltpu
from jax.sharding import PartitionSpec as P

SEQS = 1
norm_eps = 1e-05
MESH = pl.DeviceIdType.MESH

NX, NY, NZ, NC = 4, 4, 8, 2
PLANE = NX * NY * NC
COLS = 512
GU_ROWS = 32
D_ROWS = 64
WINDOW = 6


def step_kernel(
    x_ref,
    gain_ref,
    ids_ref,
    logits_ref,
    share_ref,
    taps_ref,
    og_hbm,
    ig_hbm,
    val_hbm,
    block_hbm,
    gate_hbm,
    up_hbm,
    down_hbm,
    mixer_ref,
    out_ref,
    normed,
    combine,
    outgoing,
    rows,
    gu,
    down,
    acc,
    hidden,
    results,
    returned,
    og,
    ig,
    val,
    gated,
    tail,
    halo,
    mixed,
    project_w,
    mixer_acc,
    w_sem,
    w_send,
    x_recv,
    x_send,
    r_recv,
    r_send,
    in_sem,
    halo_sem,
    share_sem,
    ring_recv,
    ring_send,
    pair_recv,
    pair_send,
    along_recv,
    along_send,
):
    tokens, width = x_ref.shape
    cap = outgoing.shape[1] // PLANE
    chunks = width // COLS
    inner = hidden.shape[1]
    gu_hops = width // GU_ROWS
    d_hops = inner // D_ROWS
    rows_mix = og.shape[0]
    split, plain = width // 2, width // 4
    part, wide = split // NZ, (width - split - plain) // NX

    ep, tp = lax.axis_index("ep"), lax.axis_index("tp")
    z, x = lax.div(ep, NX), lax.rem(ep, NX)
    y, c = lax.div(tp, NC), lax.rem(tp, NC)
    me = (c * NY + y) * NX + x
    ahead = lax.rem(z + 1, NZ) * NX + x
    behind = lax.rem(z + NZ - 1, NZ) * NX + x
    dist = lax.rem(z + NZ - (y + NY * c), NZ)
    is_home = dist == 0
    pair = y * NC + 1 - c
    n_ep, n_tp = NZ * NX, NY * NC
    flat = ep * n_tp + tp
    later = lax.rem(flat + 1, n_ep * n_tp)
    sooner = lax.rem(flat + n_ep * n_tp - 1, n_ep * n_tp)

    def peer(step):
        px = lax.rem(x + lax.rem(step, NX), NX)
        py = lax.rem(y + lax.rem(lax.div(step, NX), NY), NY)
        pc = lax.rem(c + lax.div(step, NX * NY), NC)
        return (pc * NY + py) * NX + px, z * NX + px, py * NC + pc

    def send(src, dst, send_sem, recv_sem, to):
        pltpu.make_async_remote_copy(
            src_ref=src,
            dst_ref=dst,
            send_sem=send_sem,
            recv_sem=recv_sem,
            device_id=to,
            device_id_type=MESH,
        ).start()

    def settle(ref, sem):
        pltpu.make_async_copy(ref, ref, sem).wait()

    def gu_at(i):
        return gu.at[pl.ds(pl.multiple_of(i * GU_ROWS, GU_ROWS), GU_ROWS), :]

    def down_at(j, i):
        return down.at[j, pl.ds(pl.multiple_of(i * D_ROWS, D_ROWS), D_ROWS), :]

    barrier = pltpu.get_barrier_semaphore()

    def greet(step, _):
        _, pep, ptp = peer(step)
        pl.semaphore_signal(barrier, inc=1, device_id=(pep, ptp), device_id_type=MESH)
        return 0

    lax.fori_loop(1, PLANE, greet, 0)
    for other in (ahead, behind):
        pl.semaphore_signal(barrier, inc=1, device_id=(other, tp), device_id_type=MESH)
    for other in (later, sooner):
        pl.semaphore_signal(
            barrier, inc=1, device_id=(lax.div(other, n_tp), lax.rem(other, n_tp)), device_id_type=MESH
        )

    @pl.when(is_home)
    def _():
        def load_gu(i, _):
            at = pl.ds(pl.multiple_of(i * GU_ROWS, GU_ROWS), GU_ROWS)
            pltpu.make_async_copy(gate_hbm.at[0, at, :], gu.at[at, pl.ds(0, inner)], w_sem.at[i]).start()
            pltpu.make_async_copy(up_hbm.at[0, at, :], gu.at[at, pl.ds(inner, inner)], w_sem.at[i]).start()
            return 0

        lax.fori_loop(0, gu_hops, load_gu, 0)
        for j in range(chunks):
            for i in range(d_hops):
                pltpu.make_async_copy(
                    down_hbm.at[0, pl.ds(i * D_ROWS, D_ROWS), pl.ds(j * COLS, COLS)],
                    down.at[j, pl.ds(i * D_ROWS, D_ROWS), :],
                    w_sem.at[gu_hops + j * d_hops + i],
                ).start()

    loads = [
        pltpu.make_async_copy(ig_hbm, ig, in_sem.at[0]),
        pltpu.make_async_copy(val_hbm, val, in_sem.at[1]),
        pltpu.make_async_copy(og_hbm, og, in_sem.at[2]),
        pltpu.make_async_copy(block_hbm, project_w.at[tp], in_sem.at[3]),
    ]
    for load in loads:
        load.start()

    xf = x_ref[...].astype(jnp.float32)
    scale = lax.rsqrt(jnp.mean(xf * xf, axis=-1, keepdims=True) + norm_eps)
    normed[...] = (xf * scale * gain_ref[...]).astype(jnp.bfloat16)

    loads[0].wait()
    loads[1].wait()
    product = (ig[...].astype(jnp.float32) * val[...].astype(jnp.float32)).astype(jnp.bfloat16)
    tail[...] = product[rows_mix - 16 :, :]
    gated[8:, :] = product.astype(jnp.float32)

    expert_sub = lax.broadcasted_iota(jnp.int32, (PLANE, tokens), 0)
    t_sub = lax.broadcasted_iota(jnp.int32, (tokens, tokens), 0)
    t_lane = lax.broadcasted_iota(jnp.int32, (tokens, tokens), 1)
    earlier = jnp.where(t_sub < t_lane, 1.0, 0.0).astype(jnp.bfloat16)
    id0, id1 = ids_ref[0:1, :], ids_ref[1:2, :]
    hot0 = jnp.where(expert_sub == id0, 1.0, 0.0)
    hot1 = jnp.where(expert_sub == id1, 1.0, 0.0)
    before0 = jnp.dot(hot0.astype(jnp.bfloat16), earlier, preferred_element_type=jnp.float32)
    before1 = jnp.dot(hot1.astype(jnp.bfloat16), earlier, preferred_element_type=jnp.float32)
    before1 = before1 + jnp.sum(hot0, axis=1, keepdims=True)
    slot0 = jnp.sum(hot0 * before0, axis=0, keepdims=True)
    slot1 = jnp.sum(hot1 * before1, axis=0, keepdims=True)
    place0 = id0 * cap + slot0.astype(jnp.int32)
    place1 = id1 * cap + slot1.astype(jnp.int32)

    def fill(k):
        for block in range(PLANE * cap // 256):
            row = block * 256 + lax.broadcasted_iota(jnp.int32, (256, tokens), 0)
            hit = jnp.logical_or(row == place0, row == place1)
            outgoing[k, block * 256 : (block + 1) * 256, :] = jnp.dot(
                jnp.where(hit, 1.0, 0.0).astype(jnp.bfloat16),
                normed[:, k * COLS : (k + 1) * COLS],
                preferred_element_type=jnp.float32,
            ).astype(jnp.bfloat16)

    mine = pl.ds(pl.multiple_of(me * cap, cap), cap)

    def exchange(src, dst, k, send_sem, recv_sem):
        dst[k, mine, :] = src[k, mine, :]

        def one(step, _):
            j, pep, ptp = peer(step)
            send(
                src.at[k, pl.ds(pl.multiple_of(j * cap, cap), cap), :],
                dst.at[k, mine, :],
                send_sem.at[k],
                recv_sem.at[k],
                (pep, ptp),
            )
            return 0

        lax.fori_loop(1, PLANE, one, 0)

    def all_of(ref, k, sem):
        settle(ref.at[k, pl.ds(0, (PLANE - 1) * cap), :], sem.at[k])

    half = NZ // 2

    def pass_on(piece, t, sem):
        def one(number, other, way):
            slot = lax.rem(number, WINDOW)

            @pl.when(number >= WINDOW)
            def _():
                settle(piece, w_send.at[way, slot])

            send(piece, piece, w_send.at[way, slot], sem, (other, tp))

        for all_way, some_way, other, way in (
            (dist < half - 1, dist == half - 1, ahead, 0),
            (jnp.logical_or(dist == 0, dist > half + 1), dist == half + 1, behind, 1),
        ):

            @pl.when(all_way)
            def _():
                one(t, other, way)

            @pl.when(jnp.logical_and(some_way, lax.rem(t, 2) == way))
            def _():
                one(lax.div(t, 2), other, way)

    def serve(start, stop):
        def gate_up(t, _):
            settle(gu_at(t), w_sem.at[t])
            pass_on(gu_at(t), t, w_sem.at[t])
            return 0

        def downward(t, _):
            j, i = lax.div(t - gu_hops, d_hops), lax.rem(t - gu_hops, d_hops)
            settle(down_at(j, i), w_sem.at[t])
            pass_on(down_at(j, i), t, w_sem.at[t])
            return 0

        if start < gu_hops:
            lax.fori_loop(start, min(stop, gu_hops), gate_up, 0)
        if stop > gu_hops:
            lax.fori_loop(max(start, gu_hops), stop, downward, 0)

    def project(k, piece):
        def one(n, _):
            at = pl.ds(pl.multiple_of(n * 256, 256), 256)
            product = jnp.dot(rows[k, :, :], gu[k * COLS : (k + 1) * COLS, at], preferred_element_type=jnp.float32)
            if k == 0:
                acc[:, at] = product
            else:
                acc[:, at] += product
            return 0

        steps = 2 * inner // 256 // 2
        lax.fori_loop(piece * steps, (piece + 1) * steps, one, 0)

    def activate():
        def one(b, _):
            at = pl.ds(pl.multiple_of(b * 128, 128), 128)
            g, u = acc[at, 0:inner], acc[at, inner:]
            hidden[at, :] = (g * jax.nn.sigmoid(g) * u).astype(jnp.bfloat16)
            return 0

        lax.fori_loop(0, PLANE * cap // 128, one, 0)

    def produce(j):
        def one(n, _):
            at = pl.ds(pl.multiple_of(n * 256, 256), 256)
            results[j, :, at] = jnp.dot(hidden[...], down[j, :, at], preferred_element_type=jnp.float32).astype(
                jnp.bfloat16
            )
            return 0

        lax.fori_loop(0, COLS // 256, one, 0)

    def mix(j):
        all_of(returned, j, r_recv)
        total = jnp.dot(combine[0], returned[j], preferred_element_type=jnp.float32)
        total = total + jnp.dot(combine[1], returned[j], preferred_element_type=jnp.float32)
        out_ref[:, j * COLS : (j + 1) * COLS] = total.astype(jnp.bfloat16)

    def near(i):
        return lax.rem(y + 1 + i, NY) * NC + c

    def share_of(b, q):
        return project_w.at[b, pl.ds(pl.multiple_of(q * part, part), part), :]

    others = NY - 1
    three = project_w.at[0, pl.ds(0, others * part), :]
    three_wide = project_w.at[0, pl.ds(0, others * wide), :]

    def wide_of(b, q):
        return project_w.at[b, pl.ds(pl.multiple_of(split + q * wide, wide), wide), :]

    lone, whole = NZ + NX, NZ + NX + 1
    three_plain = project_w.at[0, pl.ds(0, others * plain), :]

    def plain_of(b):
        return project_w.at[b, pl.ds(width - plain, plain), :]

    def to_pair(q):
        def one(i, _):
            send(share_of(near(i), q), share_of(near(i), q), pair_send.at[q], pair_recv.at[q], (ep, pair))
            return 0

        lax.fori_loop(0, others, one, 0)

    def wide_to_pair(q):
        def one(i, _):
            send(wide_of(near(i), q), wide_of(near(i), q), pair_send.at[NZ + q], pair_recv.at[NZ + q], (ep, pair))
            return 0

        lax.fori_loop(0, others, one, 0)

    def along_x():
        settle(three_wide, share_sem.at[3])

        def one(t, _):
            far, i = lax.div(t, others), lax.rem(t, others)
            to = z * NX + lax.rem(x + 1 + far, NX)
            send(wide_of(near(i), x), wide_of(near(i), x), along_send.at[far], along_recv.at[far], (to, tp))
            return 0

        lax.fori_loop(0, (NX - 1) * others, one, 0)
        wide_to_pair(x)

    def from_x():
        for far in range(NX - 1):
            settle(three_wide, along_recv.at[far])
            wide_to_pair(lax.rem(x + NX - 1 - far, NX))

    def from_y():
        settle(three_plain, share_sem.at[5])

        def one(i, _):
            send(plain_of(near(i)), plain_of(near(i)), pair_send.at[lone], pair_recv.at[lone], (ep, pair))
            return 0

        lax.fori_loop(0, others, one, 0)

    def goes_up(i):
        return jnp.logical_or(i == 0, jnp.logical_and(i == 2, c == 0))

    def ring_send_piece(q, way, m, i):
        other = ahead if way == 0 else behind
        piece = share_of(near(i), q)
        send(piece, piece, ring_send.at[way, m, i], ring_recv.at[way, m, i], (other, tp))

    def ring_start():
        def one(i, _):
            for way in (0, 1):
                ring_send_piece(z, way, 0, i)
            return 0

        lax.fori_loop(0, others, one, 0)

    def ring_step(k):
        for way in (0, 1):
            q = lax.rem(z + NZ - k, NZ) if way == 0 else lax.rem(z + k, NZ)

            def one(i, _):
                settle(share_of(near(i), q), ring_recv.at[way, k - 1, i])
                if k < half - 1:
                    ring_send_piece(q, way, k, i)
                else:

                    @pl.when(goes_up(i) if way == 0 else jnp.logical_not(goes_up(i)))
                    def _():
                        ring_send_piece(q, way, k, i)

                return 0

            lax.fori_loop(0, others, one, 0)
            to_pair(q)

    def ring_last():
        q = lax.rem(z + half, NZ)

        def one(i, _):
            @pl.when(goes_up(i))
            def _():
                settle(share_of(near(i), q), ring_recv.at[0, half - 1, i])

            @pl.when(jnp.logical_not(goes_up(i)))
            def _():
                settle(share_of(near(i), q), ring_recv.at[1, half - 1, i])

            return 0

        lax.fori_loop(0, others, one, 0)
        to_pair(q)

    def mixer_part(begin, end, last):
        def one(b, _):
            to = pl.ds(pl.multiple_of(b * block_cols, block_cols), block_cols)
            product = jnp.dot(mixed[:, begin:end], project_w[b, begin:end, :], preferred_element_type=jnp.float32)
            if last:
                mixer_ref[:, to] = (mixer_acc[:, to] + product).astype(jnp.bfloat16)
            else:
                mixer_acc[:, to] = product
            return 0

        lax.fori_loop(0, n_tp, one, 0)

    def mixer_second():
        for q in range(NX):
            settle(three_wide, pair_recv.at[NZ + q])
        settle(three_plain, pair_recv.at[lone])
        settle(project_w.at[tp], pair_recv.at[whole])
        mixer_part(split, width, False)

    def mixer_first():
        for q in range(NZ):
            settle(three, pair_recv.at[q])
        mixer_part(0, split, True)

    block_cols = project_w.shape[2]

    first = WINDOW
    for k in range(chunks):
        fill(k)

    margin = logits_ref[0:1, :] - logits_ref[1:2, :]
    weight0 = share_ref[...] * jax.nn.sigmoid(margin)
    weight1 = share_ref[...] * jax.nn.sigmoid(-margin)
    lane_rows = jnp.concatenate(
        [
            place0.astype(jnp.float32),
            place1.astype(jnp.float32),
            weight0,
            weight1,
            jnp.zeros((124, tokens), jnp.float32),
        ],
        axis=0,
    )
    turned = lane_rows.T
    cplace0, cplace1 = turned[:, 0:1].astype(jnp.int32), turned[:, 1:2].astype(jnp.int32)
    cweight0, cweight1 = turned[:, 2:3], turned[:, 3:4]
    for block in range(PLANE * cap // 256):
        column = block * 256 + lax.broadcasted_iota(jnp.int32, (tokens, 256), 1)
        weight = jnp.where(column == cplace0, cweight0, 0.0) + jnp.where(column == cplace1, cweight1, 0.0)
        coarse = weight.astype(jnp.bfloat16)
        combine[0, :, block * 256 : (block + 1) * 256] = coarse
        combine[1, :, block * 256 : (block + 1) * 256] = (weight - coarse.astype(jnp.float32)).astype(jnp.bfloat16)

    pl.semaphore_wait(barrier, PLANE - 1 + 4)
    send(tail, halo, halo_sem.at[0], halo_sem.at[1], (lax.div(later, n_tp), lax.rem(later, n_tp)))

    @pl.when(is_home)
    def _():
        serve(0, first)

    def give_wide(i, _):
        send(wide_of(tp, x), wide_of(tp, x), share_sem.at[2], share_sem.at[3], (ep, near(i)))
        return 0

    for k in range(chunks):
        exchange(outgoing, rows, k, x_send, x_recv)
        if k == 0:
            loads[3].wait()
            lax.fori_loop(0, others, give_wide, 0)

    def give(i, _):
        send(share_of(tp, z), share_of(tp, z), share_sem.at[0], share_sem.at[1], (ep, near(i)))
        return 0

    lax.fori_loop(0, others, give, 0)

    def give_plain(i, _):
        send(plain_of(tp), plain_of(tp), share_sem.at[4], share_sem.at[5], (ep, near(i)))
        return 0

    lax.fori_loop(0, others, give_plain, 0)
    send(project_w.at[tp], project_w.at[tp], pair_send.at[whole], pair_recv.at[whole], (ep, pair))

    @pl.when(jnp.logical_not(is_home))
    def _():
        serve(0, first)

    def upto(fraction):
        return gu_hops * fraction // 32

    serve(first, upto(14))

    settle(halo, halo_sem.at[1])
    loads[2].wait()
    seq_len = n_ep * n_tp * rows_mix // SEQS
    inside = lax.rem(flat * rows_mix, seq_len) != 0
    early = halo[...].astype(jnp.float32)[8:, :]
    gated[0:8, :] = jnp.where(inside, early, 0.0)

    def filter_columns(n, _):
        at = pl.ds(pl.multiple_of(n * 256, 256), 256)
        filtered = taps_ref[0:1, at] * gated[6 : 6 + rows_mix, at]
        filtered = filtered + taps_ref[1:2, at] * gated[7 : 7 + rows_mix, at]
        filtered = filtered + taps_ref[2:3, at] * gated[8 : 8 + rows_mix, at]
        mixed[:, at] = (og[:, at].astype(jnp.float32) * filtered).astype(jnp.bfloat16)
        return 0

    lax.fori_loop(0, width // 256, filter_columns, 0)

    serve(upto(14), upto(18))
    all_of(rows, 0, x_recv)
    project(0, 0)
    serve(upto(18), upto(19))
    project(0, 1)
    serve(upto(19), upto(26))
    along_x()
    serve(upto(26), upto(30))
    all_of(rows, 1, x_recv)
    project(1, 0)
    serve(upto(30), upto(31))
    project(1, 1)
    serve(upto(31), gu_hops + d_hops // 4)
    all_of(rows, 2, x_recv)
    project(2, 0)
    serve(gu_hops + d_hops // 4, gu_hops + d_hops // 2)
    project(2, 1)
    all_of(rows, 3, x_recv)
    project(3, 0)
    serve(gu_hops + d_hops // 2, gu_hops + d_hops * 3 // 4)
    project(3, 1)
    serve(gu_hops + d_hops * 3 // 4, gu_hops + d_hops)
    activate()
    for j in range(chunks):
        if j > 0:
            serve(gu_hops + j * d_hops, gu_hops + (j + 1) * d_hops)
        if j == chunks - 1:
            settle(three, share_sem.at[1])
            ring_start()
        produce(j)
        exchange(results, returned, j, r_send, r_recv)

    to_pair(z)
    ring_step(1)
    from_x()
    ring_step(2)
    ring_step(3)
    from_y()
    mix(0)
    mixer_second()
    ring_last()
    mix(1)
    mixer_first()
    mix(2)
    for k in range(chunks):
        all_of(outgoing, k, x_send)
        all_of(results, k, r_send)
    settle(tail, halo_sem.at[0])
    settle(three, share_sem.at[0])
    settle(three_wide, share_sem.at[2])
    settle(three_plain, share_sem.at[4])
    settle(three_plain, pair_send.at[lone])
    settle(project_w.at[tp], pair_send.at[whole])
    for q in range(NX):
        settle(three_wide, pair_send.at[NZ + q])
    for far in range(NX - 1):
        settle(three_wide, along_send.at[far])

    def pairs_left(q, _):
        settle(three, pair_send.at[q])
        return 0

    lax.fori_loop(0, NZ, pairs_left, 0)

    def rings_left(i, _):
        for way in (0, 1):
            for m in range(half - 1):
                settle(share_of(0, 0), ring_send.at[way, m, i])

        @pl.when(goes_up(i))
        def _():
            settle(share_of(0, 0), ring_send.at[0, half - 1, i])

        @pl.when(jnp.logical_not(goes_up(i)))
        def _():
            settle(share_of(0, 0), ring_send.at[1, half - 1, i])

        return 0

    lax.fori_loop(0, others, rings_left, 0)

    for sends, way in (
        (dist < half, 0),
        (jnp.logical_or(dist == 0, dist > half), 1),
    ):

        @pl.when(sends)
        def _():
            for slot in range(WINDOW):
                settle(gu_at(0), w_send.at[way, slot])

    mix(3)


def local(
    out_gate,
    in_gate,
    values,
    conv_taps,
    out_weight,
    expert_input,
    norm_gain,
    expert_ids,
    route_logits,
    group_share,
    gate_weight,
    up_weight,
    down_weight,
):
    tokens, width = expert_input.shape
    inner = gate_weight.shape[2]
    rows_mix = out_gate.shape[0]
    cap = 2 * tokens * expert_ids.shape[1] // PLANE
    chunks = width // COLS
    slots = PLANE * cap
    hops = width // GU_ROWS + chunks * (inner // D_ROWS)
    vmem = pl.BlockSpec(memory_space=pltpu.VMEM)
    hbm = pl.BlockSpec(memory_space=pltpu.HBM)
    bf, dma = jnp.bfloat16, pltpu.SemaphoreType.DMA
    return pl.pallas_call(
        step_kernel,
        out_shape=(
            jax.ShapeDtypeStruct((rows_mix, width), bf),
            jax.ShapeDtypeStruct((tokens, width), bf),
        ),
        in_specs=[vmem] * 6 + [hbm] * 7,
        out_specs=(vmem, vmem),
        scratch_shapes=[
            pltpu.VMEM((tokens, width), bf),
            pltpu.VMEM((2, tokens, slots), bf),
            pltpu.VMEM((chunks, slots, COLS), bf),
            pltpu.VMEM((chunks, slots, COLS), bf),
            pltpu.VMEM((width, 2 * inner), bf),
            pltpu.VMEM((chunks, inner, COLS), bf),
            pltpu.VMEM((slots, 2 * inner), jnp.float32),
            pltpu.VMEM((slots, inner), bf),
            pltpu.VMEM((chunks, slots, COLS), bf),
            pltpu.VMEM((chunks, slots, COLS), bf),
            pltpu.VMEM((rows_mix, width), bf),
            pltpu.VMEM((rows_mix, width), bf),
            pltpu.VMEM((rows_mix, width), bf),
            pltpu.VMEM((8 + rows_mix, width), jnp.float32),
            pltpu.VMEM((16, width), bf),
            pltpu.VMEM((16, width), bf),
            pltpu.VMEM((rows_mix, width), bf),
            pltpu.VMEM((NY * NC, *out_weight.shape), bf),
            pltpu.VMEM((rows_mix, width), jnp.float32),
            dma((hops,)),
            dma((2, WINDOW)),
            dma((chunks,)),
            dma((chunks,)),
            dma((chunks,)),
            dma((chunks,)),
            dma((4,)),
            dma((2,)),
            dma((6,)),
            dma((2, NZ // 2, NY - 1)),
            dma((2, NZ // 2, NY - 1)),
            dma((NZ + NX + 2,)),
            dma((NZ + NX + 2,)),
            dma((NX - 1,)),
            dma((NX - 1,)),
        ],
        compiler_params=pltpu.CompilerParams(
            collective_id=0, has_side_effects=True, vmem_limit_bytes=48 * 1024 * 1024
        ),
        name="layer_step",
    )(*(pltpu.with_memory_space_constraint(value, pltpu.HBM) for value in (
        expert_input,
        norm_gain[None, :],
        expert_ids.T,
        route_logits.T,
        group_share[None, :],
        conv_taps,
        out_gate,
        in_gate,
        values,
        out_weight,
        gate_weight,
        up_weight,
        down_weight,
    )))


def solution(mesh):
    return jax.shard_map(
        local,
        mesh=mesh,
        in_specs=(
            P(("ep", "tp"), None),
            P(("ep", "tp"), None),
            P(("ep", "tp"), None),
            P(),
            P(None, "tp"),
            P(("ep", "tp"), None),
            P(),
            P(("ep", "tp"), None),
            P(("ep", "tp"), None),
            P(("ep", "tp")),
            P("ep", None, None),
            P("ep", None, None),
            P("ep", None, None),
        ),
        out_specs=(P(("ep", "tp"), None), P(("ep", "tp"), None)),
        check_vma=False,
    )
```
